256 devices in a mesh: ep: 64 (over z, y, core), tp: 4 (over x).
Axes of the slice: x: 4, y: 4, z: 8, core: 2. Of those that a mesh axis runs over, the one named last changes fastest.
Arguments:
- resid: bfloat16 [2048, 2048], P('ep'), may hold values from -6 to 6
- mix_gain: bfloat16 [2048], replicated, may hold values from 0.099609375 to 1.8984375
- proj_x: bfloat16 [2048, 512], P(None, 'tp'), may hold values from -0.125 to 0.125
- proj_z: bfloat16 [2048, 512], P(None, 'tp'), may hold values from -0.125 to 0.125
- proj_b: bfloat16 [2048, 512], P(None, 'tp'), may hold values from -0.125 to 0.125
- proj_c: bfloat16 [2048, 512], P(None, 'tp'), may hold values from -0.125 to 0.125
- proj_step: bfloat16 [2048, 8], replicated, may hold values from -0.125 to 0.125
- step_bias: float32 [8], P('tp'), may hold values from -5 to -1
- decay_rate: float32 [8], P('tp'), may hold values from 1 to 16
- conv_taps: bfloat16 [3, 4, 512], P(None, None, 'tp'), may hold values from -3 to 3
- conv_state: bfloat16 [2048, 3, 3, 512], P('ep', None, None, 'tp'), may hold values from -6 to 6
- scan_state: float32 [2048, 8, 64, 128], P('ep', 'tp'), may hold values from -2.5 to 2.5
- inner_gain: bfloat16 [512], P('tp'), may hold values from 0.099609375 to 1.8984375
- proj_out: bfloat16 [512, 2048], P('tp'), may hold values from -0.25 to 0.25
- post_gain: bfloat16 [2048], replicated, may hold values from 0.099609375 to 1.8984375
- ffn_gain: bfloat16 [2048], replicated, may hold values from 0.099609375 to 1.8984375
- group_router: bfloat16 [2048, 2], replicated, may hold values from -0.125 to 0.125
- expert_router: bfloat16 [2048, 64], replicated, may hold values from -0.125 to 0.125
- route_experts: int32 [2048, 4], P('ep'), may hold values from 0 to 63, as said below
- expert_gate: bfloat16 [64, 2048, 1024], P('ep', None, 'tp'), may hold values from -0.125 to 0.125
- expert_up: bfloat16 [64, 2048, 1024], P('ep', None, 'tp'), may hold values from -0.125 to 0.125
- expert_down: bfloat16 [64, 1024, 2048], P('ep', 'tp')
- dense_switch: bfloat16 [2048], replicated, may hold values from -0.125 to 0.125
- dense_gate: bfloat16 [2048, 2048], P('ep', 'tp'), may hold values from -0.125 to 0.125
- dense_up: bfloat16 [2048, 2048], P('ep', 'tp'), may hold values from -0.125 to 0.125
- dense_down: bfloat16 [2048, 2048], P('ep', 'tp')
- out_gain: bfloat16 [2048], P('tp'), may hold values from 0.099609375 to 1.8984375
Outputs:
- layer_out: bfloat16 [2048, 2048], P('ep', 'tp')
- new_state: float32 [2048, 8, 64, 128], P('ep', 'tp')
- new_conv: bfloat16 [2048, 3, 3, 512], P('ep', None, None, 'tp')
The draws below stay inside these ranges and needn't reach their ends.
Inputs may be any that keep to these rules, and one draw needn't show every extreme that they name: `route_experts`: each row names 4 different experts, all from one group of 32 consecutive expert numbers. Within each aligned block of 32 rows (the rows of one index of ep) no expert is named more than 4 times, and one expert, the same in every block, is named exactly 4 times in every block.
All inputs are finite; a program needn't handle non-finite values.
Results may differ from the reference program's by a relative error of at most 0.019.
Values may be sent and summed in bfloat16 or wider, within the bound.
No kernel may reach another device: no remote copies, remote signals or barrier semaphores. Data moves between devices by JAX's collectives and lax.ppermute only.
A program may use at most 64 MiB of HBM per device.

```python
import math
import jax
import jax.numpy as jnp
from jax import lax

MODEL_WIDTH = 2048
HEAD_COUNT = 8
HEAD_DIM = 64
STATE_DIM = 128
STATE_GROUPS = 4
CONV_TAPS = 4
EXPERT_WIDTH = 1024
DENSE_WIDTH = 2048
ROUTE_GROUPS = 2
ROUTE_PICKS = 4
SEQ_DEV = 32
INNER_WIDTH = 512
EXPERTS = 64
GROUP_EXPERTS = 32
CAPACITY = 4
TOKENS = 2048
N_TP = 4


def draw_route_experts(key, part):
    blocks = TOKENS // SEQ_DEV
    hot_key, block_key = jax.random.split(jax.random.fold_in(key, 11))
    hot = jax.random.randint(hot_key, (), 0, EXPERTS)
    hot_group = hot // GROUP_EXPERTS
    hot_local = hot % GROUP_EXPERTS
    needed = (CAPACITY - 1) * GROUP_EXPERTS // ROUTE_PICKS + 1

    def one_block(index):
        keys = jax.random.split(jax.random.fold_in(block_key, index), 5)
        hot_rows = jax.random.randint(keys[0], (), needed, SEQ_DEV + 1)
        other = jax.random.randint(keys[1], (SEQ_DEV,), 0, ROUTE_GROUPS - 1)
        other = other + (other >= hot_group).astype(jnp.int32)
        position = jnp.arange(SEQ_DEV)
        group_of = jnp.where(position < hot_rows, hot_group, other)
        group_of = jax.random.permutation(keys[2], group_of)
        member = (group_of[:, None] == jnp.arange(ROUTE_GROUPS)[None, :]).astype(jnp.int32)
        rank = jnp.sum((jnp.cumsum(member, axis=0) - member) * member, axis=1)
        orders = jax.vmap(lambda inner: jax.random.permutation(inner, GROUP_EXPERTS))(jax.random.split(keys[3], ROUTE_GROUPS))
        offsets = jax.random.randint(keys[4], (ROUTE_GROUPS,), 0, GROUP_EXPERTS)
        hot_place = jnp.argmax((orders[hot_group] == hot_local).astype(jnp.int32))
        offsets = offsets.at[hot_group].set(hot_place)
        order_rows = orders[group_of]
        places = (offsets[group_of][:, None] + rank[:, None] * ROUTE_PICKS + jnp.arange(ROUTE_PICKS)[None, :]) % GROUP_EXPERTS
        local = jnp.take_along_axis(order_rows, places, axis=1)
        return (group_of[:, None] * GROUP_EXPERTS + local).astype(jnp.int32)
    return jax.vmap(one_block)(jnp.arange(blocks)).reshape(TOKENS, ROUTE_PICKS)


def column_ramp(width):
    ramp = jnp.arange(width, dtype=jnp.float32) / width
    return 0.5 * jnp.power(10.0, ramp)


def draw_expert_down(key, part):
    base = jax.random.truncated_normal(jax.random.fold_in(key, 21), -6.0, 6.0, (EXPERTS, EXPERT_WIDTH, MODEL_WIDTH), jnp.float32)
    base = base * EXPERT_WIDTH ** (-0.5)
    return (base * column_ramp(MODEL_WIDTH)[None, None, :]).astype(jnp.bfloat16)


def draw_dense_down(key, part):
    base = jax.random.truncated_normal(jax.random.fold_in(key, 31), -6.0, 6.0, (DENSE_WIDTH, MODEL_WIDTH), jnp.float32)
    base = base * DENSE_WIDTH ** (-0.5)
    return (base * column_ramp(MODEL_WIDTH)[None, :]).astype(jnp.bfloat16)


def shard_levels(own_key, shape, shards, smallest, top_value):
    level, own = 1.0, jax.random.fold_in(own_key, 6)
    for dim, blocks in shards:
        heights = jnp.exp(jax.random.uniform(jax.random.fold_in(own, dim), (blocks,), jnp.float32, smallest / len(shards), top_value / len(shards)))
        level = level * jnp.repeat(heights, shape[dim] // blocks).reshape([-1 if axis == dim else 1 for axis in range(len(shape))])
    return level


def normal_values(stream_key, extent, scale, limit, shards=(), held_as=jnp.bfloat16):
    values = jax.random.normal(stream_key, extent, jnp.float32) * scale
    if len(shards) > 0:
        values = shard_levels(stream_key, extent, shards, -0.22, 0.18) * values
    return jnp.clip(values, min=-limit, max=limit).astype(held_as)


def setup_inputs(seed: int = 0) -> dict:
    key_of = jax.random.split(jax.random.key(seed), 28)
    resid = normal_values(key_of[0], (TOKENS, MODEL_WIDTH), 1.0, 6.0, ((0, 64),))
    mix_gain = jnp.clip(1.0 + 0.18 * jax.random.normal(key_of[1], (MODEL_WIDTH,), jnp.float32), 0.099609375, 1.8984375).astype(jnp.bfloat16)
    proj_x = normal_values(key_of[2], (MODEL_WIDTH, INNER_WIDTH), MODEL_WIDTH ** -0.5, 0.125, ((1, 4),))
    proj_z = normal_values(key_of[3], (MODEL_WIDTH, INNER_WIDTH), MODEL_WIDTH ** -0.5, 0.125, ((1, 4),))
    proj_b = normal_values(key_of[4], (MODEL_WIDTH, STATE_GROUPS * STATE_DIM), MODEL_WIDTH ** -0.5, 0.125, ((1, 4),))
    proj_c = normal_values(key_of[5], (MODEL_WIDTH, STATE_GROUPS * STATE_DIM), MODEL_WIDTH ** -0.5, 0.125, ((1, 4),))
    proj_step = normal_values(key_of[6], (MODEL_WIDTH, HEAD_COUNT), MODEL_WIDTH ** -0.5, 0.125)
    step_bias = jnp.clip(-5.0 + 4.0 * jax.random.uniform(key_of[7], (HEAD_COUNT,), jnp.float32) ** shard_levels(key_of[7], (HEAD_COUNT,), ((0, 4),), -0.2, 0.2), -5.0, -1.0)
    decay_rate = jnp.clip(jnp.exp(math.log(16.0) - 2.7725887 * jax.random.uniform(key_of[8], (HEAD_COUNT,), jnp.float32) ** shard_levels(key_of[8], (HEAD_COUNT,), ((0, 4),), -0.2, 0.2)), 1.0, 16.0)
    conv_taps = normal_values(key_of[9], (3, CONV_TAPS, INNER_WIDTH), CONV_TAPS ** -0.5, 3.0, ((2, 4),))
    conv_state = normal_values(key_of[10], (TOKENS, 3, CONV_TAPS - 1, INNER_WIDTH), 1.0, 6.0, ((0, 64), (3, 4)))
    scan_state = normal_values(key_of[11], (TOKENS, HEAD_COUNT, HEAD_DIM, STATE_DIM), 0.3, 2.5, ((0, 64), (1, 4)), jnp.float32)
    inner_gain = jnp.clip(1.0 + 0.18 * jax.random.normal(key_of[12], (INNER_WIDTH,), jnp.float32), 0.099609375, 1.8984375).astype(jnp.bfloat16)
    proj_out = normal_values(key_of[13], (INNER_WIDTH, MODEL_WIDTH), INNER_WIDTH ** -0.5, 0.25, ((0, 4),))
    post_gain = jnp.clip(1.0 + 0.18 * jax.random.normal(key_of[14], (MODEL_WIDTH,), jnp.float32), 0.099609375, 1.8984375).astype(jnp.bfloat16)
    ffn_gain = jnp.clip(1.0 + 0.18 * jax.random.normal(key_of[15], (MODEL_WIDTH,), jnp.float32), 0.099609375, 1.8984375).astype(jnp.bfloat16)
    group_router = normal_values(key_of[16], (MODEL_WIDTH, ROUTE_GROUPS), MODEL_WIDTH ** -0.5, 0.125)
    expert_router = normal_values(key_of[17], (MODEL_WIDTH, EXPERTS), MODEL_WIDTH ** -0.5, 0.125)
    route_experts = draw_route_experts(jax.random.fold_in(key_of[27], 71), 0)
    expert_gate = normal_values(key_of[19], (EXPERTS, MODEL_WIDTH, EXPERT_WIDTH), MODEL_WIDTH ** -0.5, 0.125, ((0, 64), (2, 4)))
    expert_up = normal_values(key_of[20], (EXPERTS, MODEL_WIDTH, EXPERT_WIDTH), MODEL_WIDTH ** -0.5, 0.125, ((0, 64), (2, 4)))
    expert_down = draw_expert_down(jax.random.fold_in(key_of[27], 71), 0)
    dense_switch = normal_values(key_of[22], (MODEL_WIDTH,), MODEL_WIDTH ** -0.5, 0.125)
    dense_gate = normal_values(key_of[23], (DENSE_WIDTH, MODEL_WIDTH), MODEL_WIDTH ** -0.5, 0.125, ((0, 64), (1, 4)))
    dense_up = normal_values(key_of[24], (DENSE_WIDTH, MODEL_WIDTH), MODEL_WIDTH ** -0.5, 0.125, ((0, 64), (1, 4)))
    dense_down = draw_dense_down(jax.random.fold_in(key_of[27], 71), 0)
    out_gain = jnp.clip(1.0 + 0.18 * jax.random.normal(key_of[26], (MODEL_WIDTH,), jnp.float32), 0.099609375, 1.8984375).astype(jnp.bfloat16)
    return dict(resid=resid, mix_gain=mix_gain, proj_x=proj_x, proj_z=proj_z, proj_b=proj_b, proj_c=proj_c, proj_step=proj_step, step_bias=step_bias, decay_rate=decay_rate, conv_taps=conv_taps, conv_state=conv_state, scan_state=scan_state, inner_gain=inner_gain, proj_out=proj_out, post_gain=post_gain, ffn_gain=ffn_gain, group_router=group_router, expert_router=expert_router, route_experts=route_experts, expert_gate=expert_gate, expert_up=expert_up, expert_down=expert_down, dense_switch=dense_switch, dense_gate=dense_gate, dense_up=dense_up, dense_down=dense_down, out_gain=out_gain)


norm_eps = 1e-06

def scaled_rows(values, gain):
    values = values.astype(jnp.float32)
    mean_square = lax.optimization_barrier(jnp.mean(values * values, axis=-1, keepdims=True))
    return values * lax.rsqrt(mean_square + norm_eps) * gain.astype(jnp.float32)

def softmax_plain(logits):
    weights = jnp.exp(logits)
    return weights / lax.optimization_barrier(jnp.sum(weights, axis=-1, keepdims=True))

def state_block(pieces):
    old_state, keep, driven, b_heads, c_heads = pieces
    updated = keep[:, :, None, None] * old_state + driven[:, :, :, None] * b_heads[:, :, None, :]
    read = lax.optimization_barrier(jnp.sum(updated * c_heads[:, :, None, :], axis=3))
    return (updated, read)

def expert_block(pieces):
    rows, gate_weight, up_weight, down_weight = pieces
    gate_value = jnp.dot(rows, gate_weight, preferred_element_type=jnp.float32)
    up_value = jnp.dot(rows, up_weight, preferred_element_type=jnp.float32)
    hidden = (jax.nn.silu(gate_value) * up_value).astype(jnp.bfloat16)
    share = hidden.shape[1] // N_TP
    parts = jnp.einsum('rqf,qfd->qrd', hidden.reshape(rows.shape[0], N_TP, share).astype(jnp.float32), down_weight.reshape(N_TP, share, down_weight.shape[1]).astype(jnp.float32))
    parts = lax.optimization_barrier(parts.astype(jnp.bfloat16))
    return lax.optimization_barrier(jnp.sum(parts.astype(jnp.float32), axis=0)).astype(jnp.bfloat16)

def reference(resid, mix_gain, proj_x, proj_z, proj_b, proj_c, proj_step, step_bias, decay_rate, conv_taps, conv_state, scan_state, inner_gain, proj_out, post_gain, ffn_gain, group_router, expert_router, route_experts, expert_gate, expert_up, expert_down, dense_switch, dense_gate, dense_up, dense_down, out_gain):
    normed = scaled_rows(resid, mix_gain).astype(jnp.bfloat16)
    fresh = jnp.stack([jnp.dot(normed, proj_x, preferred_element_type=jnp.float32), jnp.dot(normed, proj_b, preferred_element_type=jnp.float32), jnp.dot(normed, proj_c, preferred_element_type=jnp.float32)], axis=1).astype(jnp.bfloat16)
    gate_z = jnp.dot(normed, proj_z, preferred_element_type=jnp.float32)
    step_raw = jnp.dot(normed, proj_step, preferred_element_type=jnp.float32)
    history = jnp.concatenate([conv_state, fresh[:, :, None, :]], axis=2)
    activated = jax.nn.silu(lax.optimization_barrier(jnp.sum(history.astype(jnp.float32) * conv_taps.astype(jnp.float32)[None], axis=2)))
    repeat = HEAD_COUNT // STATE_GROUPS
    xs_heads = activated[:, 0].reshape(TOKENS, HEAD_COUNT, HEAD_DIM)
    b_heads = jnp.repeat(activated[:, 1].reshape(TOKENS, STATE_GROUPS, STATE_DIM), repeat, axis=1)
    c_heads = jnp.repeat(activated[:, 2].reshape(TOKENS, STATE_GROUPS, STATE_DIM), repeat, axis=1)
    step = jax.nn.softplus(step_raw + step_bias)
    keep = jnp.exp(-decay_rate * step)
    driven = step[:, :, None] * xs_heads
    blocks = TOKENS // SEQ_DEV

    def by_block(array):
        return array.reshape((blocks, SEQ_DEV) + array.shape[1:])
    new_state, read = lax.map(state_block, (by_block(scan_state), by_block(keep), by_block(driven), by_block(b_heads), by_block(c_heads)))
    new_state = new_state.reshape(scan_state.shape)
    read = read.reshape(TOKENS, INNER_WIDTH)
    gated = (read * jax.nn.silu(gate_z) * inner_gain.astype(jnp.float32)).astype(jnp.bfloat16)
    mixed = jnp.dot(gated, proj_out, preferred_element_type=jnp.float32)
    stream = (resid.astype(jnp.float32) + scaled_rows(mixed, post_gain)).astype(jnp.bfloat16)
    feed = scaled_rows(stream, ffn_gain).astype(jnp.bfloat16)
    group_prob = softmax_plain(jnp.dot(feed, group_router, preferred_element_type=jnp.float32))
    expert_logits = jnp.dot(feed, expert_router, preferred_element_type=jnp.float32)
    matches = route_experts[:, :, None] == jnp.arange(EXPERTS, dtype=jnp.int32)[None, None, :]
    pick_logits = lax.optimization_barrier(jnp.sum(jnp.where(matches, expert_logits[:, None, :], 0.0), axis=2))
    chosen_group = route_experts[:, 0] // GROUP_EXPERTS
    group_weight = lax.optimization_barrier(jnp.sum(jnp.where(chosen_group[:, None] == jnp.arange(ROUTE_GROUPS, dtype=jnp.int32)[None, :], group_prob, 0.0), axis=1))
    pick_weight = softmax_plain(pick_logits) * group_weight[:, None]
    flat_picks = route_experts.reshape(blocks, SEQ_DEV * ROUTE_PICKS)
    one_hot = (flat_picks[:, :, None] == jnp.arange(EXPERTS, dtype=jnp.int32)[None, None, :]).astype(jnp.int32)
    slot = lax.optimization_barrier(jnp.sum((jnp.cumsum(one_hot, axis=1) - one_hot) * one_hot, axis=2))
    block_ids = jnp.arange(blocks, dtype=jnp.int32)[:, None]
    target = ((flat_picks * blocks + block_ids) * CAPACITY + slot).reshape(-1).astype(jnp.int32)
    repeated = jnp.repeat(feed, ROUTE_PICKS, axis=0)
    buffer = jnp.zeros((EXPERTS * blocks * CAPACITY, MODEL_WIDTH), jnp.bfloat16).at[target].set(repeated)
    served = lax.map(expert_block, (buffer.reshape(EXPERTS, blocks * CAPACITY, MODEL_WIDTH), expert_gate, expert_up, expert_down))
    expert_out = served.reshape(-1, MODEL_WIDTH)[target].reshape(TOKENS, ROUTE_PICKS, MODEL_WIDTH)
    routed = lax.optimization_barrier(jnp.sum(expert_out.astype(jnp.float32) * pick_weight[:, :, None], axis=1))
    dense_pre_gate = jnp.dot(feed, dense_gate.T, preferred_element_type=jnp.float32)
    dense_pre_up = jnp.dot(feed, dense_up.T, preferred_element_type=jnp.float32)
    dense_hidden = (jax.nn.silu(dense_pre_gate) * dense_pre_up).astype(jnp.bfloat16)
    dense_out = jnp.dot(dense_hidden, dense_down, preferred_element_type=jnp.float32)
    switch = jax.nn.sigmoid(jnp.dot(feed, dense_switch, preferred_element_type=jnp.float32))
    combined = routed + switch[:, None] * dense_out
    layer_out = (stream.astype(jnp.float32) + scaled_rows(combined, out_gain)).astype(jnp.bfloat16)
    new_conv = history[:, :, 1:, :]
    return (layer_out, new_state, new_conv)
```

```python
import jax
import jax.numpy as jnp
from jax import lax
from jax.sharding import Mesh
from jax.sharding import PartitionSpec as P

EP = ("ep_0", "ep_1", "ep_2")
YC = ("ep_1", "ep_2")


norm_eps = 1e-06


def from_shift(array, axis, shift):
    count = lax.axis_size(axis)
    return lax.ppermute(array, axis, [(i, (i + shift) % count) for i in range(count)])


def from_all(array, axis):
    count = lax.axis_size(axis)
    return [array] + [from_shift(array, axis, s) for s in range(1, count)]


def scaled_rows(values, gain):
    values = values.astype(jnp.float32)
    mean_square = jnp.mean(values * values, axis=-1, keepdims=True)
    return values * lax.rsqrt(mean_square + norm_eps) * gain.astype(jnp.float32)


def dot32(a, b):
    return jnp.dot(a, b, preferred_element_type=jnp.float32)


def sum_of(arrays):
    total = arrays[0].astype(jnp.float32)
    for array in arrays[1:]:
        total = total + array.astype(jnp.float32)
    return total


def on_device(
    resid,
    mix_gain,
    proj_x,
    proj_z,
    proj_b,
    proj_c,
    proj_step,
    step_bias,
    decay_rate,
    conv_taps,
    conv_state,
    scan_state,
    inner_gain,
    proj_out,
    post_gain,
    ffn_gain,
    group_router,
    expert_router,
    route_experts,
    expert_gate,
    expert_up,
    expert_down,
    dense_switch,
    dense_gate,
    dense_up,
    dense_down,
    out_gain,
):
    tp_index = lax.axis_index("tp")
    tp_count = lax.axis_size("tp")
    seqs, width = resid.shape
    quarter = width // tp_count
    heads_here, head_dim, state_dim = scan_state.shape[1:]
    channels = conv_state.shape[3]
    repeat = heads_here // (channels // state_dim)
    units = dense_gate.shape[0]

    rows_of_units = jnp.stack([dense_gate, dense_up, dense_down])
    unit_blocks = from_all(rows_of_units, "ep_0")
    down = expert_down[0]
    down_parts = [
        lax.dynamic_slice_in_dim(down, ((tp_index + s) % tp_count) * quarter, quarter, 1)
        for s in range(tp_count)
    ]
    down_parts = [down_parts[0]] + [
        from_shift(down_parts[s], "tp", s) for s in range(1, tp_count)
    ]

    expert_count = expert_router.shape[1]
    group_size = expert_count // group_router.shape[1]
    pick_count = route_experts.shape[1]
    capacity = 2 * seqs * pick_count // expert_count
    experts = jnp.arange(expert_count, dtype=jnp.int32)
    picked = jnp.any(route_experts[:, :, None] == experts[None, None, :], axis=1)
    earlier = jnp.tril(jnp.ones((seqs, seqs), jnp.float32), -1)
    slot = dot32(earlier, picked.astype(jnp.float32))
    in_slot = picked[:, :, None] & (
        slot[:, :, None] == jnp.arange(capacity, dtype=jnp.float32)[None, None, :]
    )
    in_slot = in_slot.reshape(seqs, expert_count * capacity)

    normed = scaled_rows(resid, mix_gain).astype(jnp.bfloat16)
    fresh = jnp.stack(
        [dot32(normed, proj_x), dot32(normed, proj_b), dot32(normed, proj_c)], axis=1
    ).astype(jnp.bfloat16)
    gate_z = dot32(normed, proj_z)
    step_all = dot32(normed, proj_step)
    step_raw = lax.dynamic_slice_in_dim(step_all, tp_index * heads_here, heads_here, 1)
    history = jnp.concatenate([conv_state, fresh[:, :, None, :]], axis=2)
    activated = jax.nn.silu(
        jnp.sum(history.astype(jnp.float32) * conv_taps.astype(jnp.float32)[None], axis=2)
    )
    xs_heads = activated[:, 0].reshape(seqs, heads_here, head_dim)
    b_heads = jnp.repeat(activated[:, 1].reshape(seqs, -1, state_dim), repeat, axis=1)
    c_heads = jnp.repeat(activated[:, 2].reshape(seqs, -1, state_dim), repeat, axis=1)
    step = jax.nn.softplus(step_raw + step_bias)
    keep = jnp.exp(-decay_rate * step)
    driven = step[:, :, None] * xs_heads
    new_state = keep[:, :, None, None] * scan_state + driven[:, :, :, None] * b_heads[:, :, None, :]
    read = jnp.sum(new_state * c_heads[:, :, None, :], axis=3).reshape(seqs, channels)
    gated = (read * jax.nn.silu(gate_z) * inner_gain.astype(jnp.float32)).astype(jnp.bfloat16)
    part = dot32(gated, proj_out).astype(jnp.bfloat16)
    mixed = sum_of(from_all(part, "tp"))
    stream = (resid.astype(jnp.float32) + scaled_rows(mixed, post_gain)).astype(jnp.bfloat16)
    feed = scaled_rows(stream, ffn_gain).astype(jnp.bfloat16)

    outgoing = lax.dot_general(
        in_slot.astype(jnp.bfloat16), feed, (((0,), (0,)), ((), ())),
        preferred_element_type=jnp.float32,
    ).astype(jnp.bfloat16)
    arrived = lax.all_to_all(
        outgoing.reshape(expert_count, capacity, width), EP, 0, 0, tiled=True
    )
    rows = arrived.reshape(expert_count * capacity, width)

    feed_quarter = lax.dynamic_slice_in_dim(feed, tp_index * quarter, quarter, 1)
    tokens = jnp.concatenate(from_all(feed_quarter, YC), axis=0)
    gate_rows = jnp.concatenate([b[0] for b in unit_blocks], axis=0)
    up_rows = jnp.concatenate([b[1] for b in unit_blocks], axis=0)
    down_rows = jnp.concatenate([b[2] for b in unit_blocks], axis=0)
    across = (((1,), (1,)), ((), ()))
    gate_piece = lax.dot_general(tokens, gate_rows, across, preferred_element_type=jnp.float32)
    up_piece = lax.dot_general(tokens, up_rows, across, preferred_element_type=jnp.float32)
    pieces = jnp.stack([gate_piece, up_piece]).astype(jnp.bfloat16)
    sums = sum_of(from_all(pieces, "tp"))
    dense_hidden = (jax.nn.silu(sums[0]) * sums[1]).astype(jnp.bfloat16)
    dense_part = dot32(dense_hidden, down_rows).astype(jnp.bfloat16)
    blocks = dense_part.shape[0] // seqs
    dense_parts = dense_part.reshape(blocks, seqs, quarter)
    dense_out = sum_of(
        [dense_parts[0]] + [from_shift(dense_parts[s], YC, -s) for s in range(1, blocks)]
    )

    gate_value = dot32(rows, expert_gate[0])
    up_value = dot32(rows, expert_up[0])
    hidden = (jax.nn.silu(gate_value) * up_value).astype(jnp.bfloat16)
    all_hidden = jnp.concatenate(from_all(hidden, "tp"), axis=1)
    served = dot32(all_hidden, jnp.concatenate(down_parts, axis=0)).astype(jnp.bfloat16)
    returned = lax.all_to_all(
        served.reshape(expert_count, capacity, quarter), EP, 0, 0, tiled=True
    ).reshape(expert_count * capacity, quarter)

    group_logits = dot32(feed, group_router)
    group_exp = jnp.exp(group_logits)
    group_prob = group_exp / jnp.sum(group_exp, axis=-1, keepdims=True)
    chosen = route_experts[:, :1] // group_size
    group_ids = jnp.arange(group_router.shape[1], dtype=jnp.int32)
    group_weight = jnp.sum(
        jnp.where(chosen == group_ids[None, :], group_prob, 0.0), axis=1, keepdims=True
    )
    logits = jnp.where(picked, dot32(feed, expert_router), -jnp.inf)
    pick_exp = jnp.exp(logits)
    pick_weight = pick_exp / jnp.sum(pick_exp, axis=-1, keepdims=True) * group_weight
    slot_weight = jnp.where(in_slot, jnp.repeat(pick_weight, capacity, axis=1), 0.0)
    weight_high = slot_weight.astype(jnp.bfloat16)
    weight_low = (slot_weight - weight_high.astype(jnp.float32)).astype(jnp.bfloat16)
    routed = dot32(weight_high, returned) + dot32(weight_low, returned)

    switch = jax.nn.sigmoid(dot32(feed, dense_switch))
    combined = routed + switch[:, None] * dense_out
    squares = jnp.sum(combined * combined, axis=1)
    total_square = sum_of(from_all(squares, "tp"))
    scale = lax.rsqrt(total_square / width + norm_eps)
    stream_part = lax.dynamic_slice_in_dim(stream, tp_index * quarter, quarter, 1).astype(
        jnp.float32
    )
    layer_out = (stream_part + combined * scale[:, None] * out_gain.astype(jnp.float32)).astype(
        jnp.bfloat16
    )
    new_conv = history[:, :, 1:, :]
    return (layer_out, new_state, new_conv)


def solution(mesh):
    torus = Mesh(mesh.devices.reshape(8, 4, 2, mesh.shape["tp"]), ("ep_0", "ep_1", "ep_2", "tp"))
    in_specs = (
        P(EP, None),
        P(),
        P(None, "tp"),
        P(None, "tp"),
        P(None, "tp"),
        P(None, "tp"),
        P(),
        P("tp"),
        P("tp"),
        P(None, None, "tp"),
        P(EP, None, None, "tp"),
        P(EP, "tp", None, None),
        P("tp"),
        P("tp", None),
        P(),
        P(),
        P(),
        P(),
        P(EP, None),
        P(EP, None, "tp"),
        P(EP, None, "tp"),
        P(EP, "tp", None),
        P(),
        P(EP, "tp"),
        P(EP, "tp"),
        P(EP, "tp"),
        P("tp"),
    )
    out_specs = (P(EP, "tp"), P(EP, "tp", None, None), P(EP, None, None, "tp"))
    return jax.shard_map(
        on_device, mesh=torus, in_specs=in_specs, out_specs=out_specs, check_vma=False
    )
```

```python
import jax
import jax.numpy as jnp
from jax import lax
from jax.sharding import Mesh
from jax.experimental import pallas as pl
from jax.experimental.pallas import tpu as pltpu
from jax.sharding import PartitionSpec as P


EP = ("ep_0", "ep_1", "ep_2")


norm_eps = 1e-06
MIXER_VMEM = 16 * 2**20


def from_shift(array, axis, shift):
    count = lax.axis_size(axis)
    return lax.ppermute(array, axis, [(i, (i + shift) % count) for i in range(count)])


def from_all(array, axis):
    count = lax.axis_size(axis)
    return [array] + [from_shift(array, axis, s) for s in range(1, count)]


def scaled_rows(values, gain):
    values = values.astype(jnp.float32)
    mean_square = jnp.mean(values * values, axis=-1, keepdims=True)
    return values * lax.rsqrt(mean_square + norm_eps) * gain.astype(jnp.float32)


def dot32(a, b):
    return jnp.dot(a, b, preferred_element_type=jnp.float32)


def sum_of(arrays):
    total = arrays[0].astype(jnp.float32)
    for array in arrays[1:]:
        total = total + array.astype(jnp.float32)
    return total


def from_flip(array, axis, bit):
    count = lax.axis_size(axis)
    return lax.ppermute(array, axis, [(i, i ^ bit) for i in range(count)])


def silu(values):
    return values * (1.0 / (1.0 + jnp.exp(-values)))


def mixer_kernel(
    place,
    step_bias,
    decay_rate,
    resid,
    mix_gain,
    proj_x,
    proj_z,
    proj_b,
    proj_c,
    proj_step,
    conv_taps,
    conv_state,
    scan_state,
    inner_gain,
    proj_out,
    routes,
    part,
    new_state,
    new_conv,
    in_slot,
):
    seqs = resid.shape[0]
    slots = in_slot.shape[0]
    slot_ids = lax.broadcasted_iota(jnp.int32, (slots, seqs), 0)
    picked = jnp.zeros((slots, seqs), jnp.bool_)
    for k in range(routes.shape[0]):
        picked = picked | ((slot_ids >> 2) == routes[k : k + 1])
    earlier = lax.broadcasted_iota(jnp.int32, (seqs, seqs), 0) < lax.broadcasted_iota(
        jnp.int32, (seqs, seqs), 1
    )
    rank = dot32(
        jnp.where(picked, 1.0, 0.0).astype(jnp.bfloat16),
        jnp.where(earlier, 1.0, 0.0).astype(jnp.bfloat16),
    )
    in_slot[...] = jnp.where(
        picked & (rank.astype(jnp.int32) == (slot_ids & 3)), 1.0, 0.0
    ).astype(jnp.bfloat16)
    heads, head_dim, lanes = scan_state.shape[1:]
    values = resid[...].astype(jnp.float32)
    mean_square = jnp.mean(values * values, axis=-1, keepdims=True)
    normed = values * lax.rsqrt(mean_square + norm_eps) * mix_gain[...].astype(jnp.float32)
    normed = normed.astype(jnp.bfloat16)
    parts = []
    for k, proj in enumerate((proj_x, proj_b, proj_c)):
        fresh = dot32(normed, proj[...]).astype(jnp.bfloat16)
        taps = conv_taps[k].astype(jnp.float32)
        total = fresh.astype(jnp.float32) * taps[3:4]
        for pos in range(3):
            total = total + conv_state[k, pos].astype(jnp.float32) * taps[pos : pos + 1]
        new_conv[k, 0] = conv_state[k, 1]
        new_conv[k, 1] = conv_state[k, 2]
        new_conv[k, 2] = fresh
        parts.append(silu(total))
    xs, bs, cs = parts
    gate = silu(dot32(normed, proj_z[...])) * inner_gain[...].astype(jnp.float32)
    step_all = lax.dot_general(
        normed, proj_step[...], (((1,), (1,)), ((), ())), preferred_element_type=jnp.float32
    )
    head_ids = lax.broadcasted_iota(jnp.int32, step_all.shape, 1)
    lane_ids = lax.broadcasted_iota(jnp.int32, (seqs, lanes), 1)
    steps, keeps = [], []
    for h in range(heads):
        raw = jnp.sum(
            jnp.where(head_ids == place[0] * heads + h, step_all, 0.0), axis=1, keepdims=True
        )
        raw = raw + step_bias[h]
        step = jnp.maximum(raw, 0.0) + jnp.log1p(jnp.exp(-jnp.abs(raw)))
        steps.append(step)
        keeps.append(jnp.exp(-decay_rate[h] * step))
    driven = xs * jnp.where(lane_ids < head_dim, steps[0], steps[1])
    filler = jnp.zeros((lanes - seqs, lanes), jnp.float32)
    driven = jnp.concatenate([driven, filler], axis=0).T
    wide_ids = lax.broadcasted_iota(jnp.int32, (head_dim, lanes), 1)
    reads = [jnp.zeros((head_dim, lanes), jnp.float32) for _ in range(heads)]
    for t in range(seqs):
        for h in range(heads):
            column = driven[h * head_dim : (h + 1) * head_dim, t : t + 1]
            state = keeps[h][t : t + 1] * scan_state[t, h] + column * bs[t : t + 1]
            new_state[t, h] = state
            read = jnp.sum(state * cs[t : t + 1], axis=1, keepdims=True)
            reads[h] = jnp.where(wide_ids == t, read, reads[h])
    read = jnp.concatenate(reads, axis=0).T[:seqs]
    gated = (read * gate).astype(jnp.bfloat16)
    part[...] = dot32(gated, proj_out[...]).astype(jnp.bfloat16)


def mixer(slots, place, step_bias, decay_rate, *arrays):
    resid, conv_state, scan_state = arrays[0], arrays[8], arrays[9]
    smem = pl.BlockSpec(memory_space=pltpu.SMEM)
    vmem = pl.BlockSpec(memory_space=pltpu.VMEM)
    return pl.pallas_call(
        mixer_kernel,
        name="mixer",
        in_specs=[smem] * 3 + [vmem] * len(arrays),
        out_specs=[vmem] * 4,
        compiler_params=pltpu.CompilerParams(vmem_limit_bytes=MIXER_VMEM),
        out_shape=[
            jax.ShapeDtypeStruct(resid.shape, jnp.bfloat16),
            jax.ShapeDtypeStruct(scan_state.shape, jnp.float32),
            jax.ShapeDtypeStruct(conv_state.shape, jnp.bfloat16),
            jax.ShapeDtypeStruct((slots, resid.shape[0]), jnp.bfloat16),
        ],
    )(place, step_bias, decay_rate, *arrays)


def feeder_kernel(
    part_0, part_1, part_2, part_3, resid, post_gain, ffn_gain, in_slot, stream, feed, outgoing
):
    mixed = sum_of([part_0[...], part_1[...], part_2[...], part_3[...]])
    total = resid[...].astype(jnp.float32) + scaled_rows(mixed, post_gain[...])
    total = total.astype(jnp.bfloat16)
    stream[...] = total
    fed = scaled_rows(total, ffn_gain[...]).astype(jnp.bfloat16)
    feed[...] = fed
    outgoing[...] = dot32(in_slot[...], fed).astype(jnp.bfloat16)


def feeder(*arrays):
    vmem = pl.BlockSpec(memory_space=pltpu.VMEM)
    rows = jax.ShapeDtypeStruct(arrays[0].shape, jnp.bfloat16)
    return pl.pallas_call(
        feeder_kernel,
        name="feeder",
        in_specs=[vmem] * len(arrays),
        out_specs=[vmem] * 3,
        compiler_params=pltpu.CompilerParams(vmem_limit_bytes=MIXER_VMEM),
        out_shape=[
            rows,
            rows,
            jax.ShapeDtypeStruct((arrays[-1].shape[0], arrays[0].shape[1]), jnp.bfloat16),
        ],
    )(*arrays)


def on_device(
    resid,
    mix_gain,
    proj_x,
    proj_z,
    proj_b,
    proj_c,
    proj_step,
    step_bias,
    decay_rate,
    conv_taps,
    conv_state,
    scan_state,
    inner_gain,
    proj_out,
    post_gain,
    ffn_gain,
    group_router,
    expert_router,
    route_experts,
    expert_gate,
    expert_up,
    expert_down,
    dense_switch,
    dense_gate,
    dense_up,
    dense_down,
    out_gain,
):
    tp_index = lax.axis_index("tp")
    tp_count = lax.axis_size("tp")
    seqs, width = resid.shape
    quarter = width // tp_count
    units = dense_gate.shape[0]

    blocks = jnp.stack([dense_gate, dense_up, dense_down])[None]
    blocks = jnp.concatenate([blocks, from_flip(blocks, "ep_0", 4)])
    blocks = jnp.concatenate([blocks, from_flip(blocks, "ep_0", 2)])
    blocks = jnp.concatenate([blocks, from_flip(blocks, "ep_0", 1)])
    unit_rows = jnp.moveaxis(blocks, 0, 1).reshape(3, blocks.shape[0] * units, quarter)
    down = expert_down[0]
    down_parts = [
        lax.dynamic_slice_in_dim(down, ((tp_index + s) % tp_count) * quarter, quarter, 1)
        for s in range(tp_count)
    ]
    down_parts = [down_parts[0]] + [from_shift(down_parts[s], "tp", s) for s in range(1, tp_count)]

    expert_count = expert_router.shape[1]
    group_size = expert_count // group_router.shape[1]
    pick_count = route_experts.shape[1]
    capacity = 2 * seqs * pick_count // expert_count

    part, new_state, new_conv, in_slot = mixer(
        expert_count * capacity,
        jnp.full((1,), tp_index, jnp.int32),
        step_bias,
        decay_rate,
        resid,
        mix_gain[None],
        proj_x,
        proj_z,
        proj_b,
        proj_c,
        proj_step.T,
        conv_taps,
        conv_state.transpose(1, 2, 0, 3),
        scan_state,
        inner_gain[None],
        proj_out,
        route_experts.T,
    )
    new_conv = new_conv.transpose(2, 0, 1, 3)
    mixed_parts = from_all(part, "tp")
    stream, feed, outgoing = feeder(*mixed_parts, resid, post_gain[None], ffn_gain[None], in_slot)

    feed_quarter = lax.dynamic_slice_in_dim(feed, tp_index * quarter, quarter, 1)
    arrived = lax.all_to_all(outgoing.reshape(expert_count, capacity, width), EP, 0, 0, tiled=True)
    rows = arrived.reshape(expert_count * capacity, width)

    tokens = jnp.concatenate([feed_quarter, from_flip(feed_quarter, "ep_2", 1)], axis=0)
    tokens = jnp.concatenate(from_all(tokens, "ep_1"), axis=0)
    gate_rows, up_rows, down_rows = unit_rows
    across = (((1,), (1,)), ((), ()))
    gate_piece = lax.dot_general(tokens, gate_rows, across, preferred_element_type=jnp.float32)
    up_piece = lax.dot_general(tokens, up_rows, across, preferred_element_type=jnp.float32)
    pieces = jnp.stack([gate_piece, up_piece]).astype(jnp.bfloat16)
    sums = sum_of(from_all(pieces, "tp"))
    dense_hidden = (jax.nn.silu(sums[0]) * sums[1]).astype(jnp.bfloat16)
    dense_part = dot32(dense_hidden, down_rows).astype(jnp.bfloat16)
    lots = dense_part.reshape(lax.axis_size("ep_1"), 2 * seqs, quarter)
    lots = sum_of([lots[0]] + [from_shift(lots[b], "ep_1", -b) for b in range(1, lots.shape[0])])
    dense_part = lots[:seqs] + from_flip(lots[seqs:].astype(jnp.bfloat16), "ep_2", 1)
    dense_out = dense_part

    gate_value = dot32(rows, expert_gate[0])
    up_value = dot32(rows, expert_up[0])
    hidden = (jax.nn.silu(gate_value) * up_value).astype(jnp.bfloat16)
    hidden_parts = from_all(hidden, "tp")
    served = sum(dot32(r, w) for r, w in zip(hidden_parts, down_parts)).astype(jnp.bfloat16)
    returned = lax.all_to_all(
        served.reshape(expert_count, capacity, quarter), EP, 0, 0, tiled=True
    ).reshape(expert_count * capacity, quarter)

    features = (((0,), (1,)), ((), ()))
    group_exp = jnp.exp(
        lax.dot_general(group_router, feed, features, preferred_element_type=jnp.float32)
    )
    group_prob = group_exp / jnp.sum(group_exp, axis=0, keepdims=True)
    routes = route_experts.T
    group_ids = jnp.arange(group_router.shape[1], dtype=jnp.int32)[:, None]
    group_weight = jnp.sum(
        jnp.where(routes[:1] // group_size == group_ids, group_prob, 0.0), axis=0, keepdims=True
    )
    expert_ids = jnp.arange(expert_count, dtype=jnp.int32)[:, None]
    picked = expert_ids == routes[0:1]
    for k in range(1, pick_count):
        picked = picked | (expert_ids == routes[k : k + 1])
    logits = lax.dot_general(expert_router, feed, features, preferred_element_type=jnp.float32)
    pick_exp = jnp.exp(jnp.where(picked, logits, -jnp.inf))
    pick_weight = pick_exp / jnp.sum(pick_exp, axis=0, keepdims=True) * group_weight
    slot_weight = in_slot.astype(jnp.float32) * jnp.repeat(pick_weight, capacity, axis=0)
    weight_high = slot_weight.astype(jnp.bfloat16)
    weight_low = (slot_weight - weight_high.astype(jnp.float32)).astype(jnp.bfloat16)
    slotwise = (((0,), (0,)), ((), ()))
    routed = lax.dot_general(
        weight_high, returned, slotwise, preferred_element_type=jnp.float32
    ) + lax.dot_general(weight_low, returned, slotwise, preferred_element_type=jnp.float32)

    switch = jax.nn.sigmoid(dot32(feed, dense_switch))
    combined = routed + switch[:, None] * dense_out
    squares = jnp.sum(combined * combined, axis=1)
    total_square = sum_of(from_all(squares, "tp"))
    scale = lax.rsqrt(total_square / width + norm_eps)
    stream_part = lax.dynamic_slice_in_dim(stream, tp_index * quarter, quarter, 1).astype(
        jnp.float32
    )
    layer_out = (stream_part + combined * scale[:, None] * out_gain.astype(jnp.float32)).astype(
        jnp.bfloat16
    )
    return (layer_out, new_state, new_conv)


def solution(mesh):
    torus = Mesh(mesh.devices.reshape(8, 4, 2, mesh.shape["tp"]), ("ep_0", "ep_1", "ep_2", "tp"))
    in_specs = (
        P(EP, None),
        P(),
        P(None, "tp"),
        P(None, "tp"),
        P(None, "tp"),
        P(None, "tp"),
        P(),
        P("tp"),
        P("tp"),
        P(None, None, "tp"),
        P(EP, None, None, "tp"),
        P(EP, "tp", None, None),
        P("tp"),
        P("tp", None),
        P(),
        P(),
        P(),
        P(),
        P(EP, None),
        P(EP, None, "tp"),
        P(EP, None, "tp"),
        P(EP, "tp", None),
        P(),
        P(EP, "tp"),
        P(EP, "tp"),
        P(EP, "tp"),
        P("tp"),
    )
    out_specs = (P(EP, "tp"), P(EP, "tp", None, None), P(EP, None, None, "tp"))

    return jax.shard_map(
        on_device, mesh=torus, in_specs=in_specs, out_specs=out_specs, check_vma=False
    )
```

```python
import jax
import jax.numpy as jnp
from jax import lax
from jax.sharding import Mesh
from jax.experimental import pallas as pl
from jax.experimental.pallas import tpu as pltpu
from jax.sharding import PartitionSpec as P


EP = ("ep_0", "ep_1", "ep_2")


norm_eps = 1e-06
FEEDER_VMEM = 16 * 2**20
STATE_CHUNKS = 4


def from_shift(array, axis, shift):
    count = lax.axis_size(axis)
    return lax.ppermute(array, axis, [(i, (i + shift) % count) for i in range(count)])


def from_all(array, axis):
    count = lax.axis_size(axis)
    return [array] + [from_shift(array, axis, s) for s in range(1, count)]


def scaled_rows(values, gain):
    values = values.astype(jnp.float32)
    mean_square = jnp.mean(values * values, axis=-1, keepdims=True)
    return values * lax.rsqrt(mean_square + norm_eps) * gain.astype(jnp.float32)


def dot32(a, b):
    return jnp.dot(a, b, preferred_element_type=jnp.float32)


def sum_of(arrays):
    total = arrays[0].astype(jnp.float32)
    for array in arrays[1:]:
        total = total + array.astype(jnp.float32)
    return total


def from_flip(array, axis, bit):
    count = lax.axis_size(axis)
    return lax.ppermute(array, axis, [(i, i ^ bit) for i in range(count)])


def silu(values):
    return values * (1.0 / (1.0 + jnp.exp(-values)))


MIXER_INPUTS = (
    "resid", "mix_gain", "routes", "proj_x", "proj_b", "proj_c", "proj_step", "conv_taps",
    "conv_state", "step_bias", "decay_rate", "scan_state", "proj_z", "inner_gain", "proj_out",
)


def in_two(values):
    high = values.astype(jnp.bfloat16).astype(jnp.float32)
    return high, values - high


def across_last(a, b):
    return lax.dot_general(a, b, (((1,), (1,)), ((), ())), preferred_element_type=jnp.float32)


def mixer_kernel(place, *refs):
    count = len(MIXER_INPUTS)
    sources, refs = refs[:count], refs[count:]
    (part, state_out, conv_out, in_slot), refs = refs[:4], refs[4:]
    held, refs = refs[:count], refs[count:]
    new_state, new_conv, keep_rows, sems, in_sems, out_sems = refs
    at = dict(zip(MIXER_INPUTS, held))
    scan_state = at["scan_state"]
    copies = {
        name: pltpu.make_async_copy(source, target, sems.at[k])
        for k, (name, source, target) in enumerate(zip(MIXER_INPUTS, sources, held))
        if name != "scan_state"
    }
    state_in = dict(zip(MIXER_INPUTS, sources))["scan_state"]

    def share(i):
        some = state_in.shape[0] // STATE_CHUNKS
        return pl.ds(i * some, some)

    def state_copy(i):
        return pltpu.make_async_copy(
            state_in.at[share(i)], scan_state.at[share(i)], in_sems.at[i]
        )

    def out_copy(i):
        return pltpu.make_async_copy(
            new_state.at[share(i)], state_out.at[share(i)], out_sems.at[i]
        )

    for name in MIXER_INPUTS:
        if name == "scan_state":
            for i in range(STATE_CHUNKS):
                state_copy(i).start()
        else:
            copies[name].start()

    seqs = part.shape[0]
    heads, head_dim, lanes = new_state.shape[1:]
    slots = in_slot.shape[0]
    copies["resid"].wait()
    copies["mix_gain"].wait()
    values = at["resid"][...].astype(jnp.float32)
    mean_square = jnp.mean(values * values, axis=-1, keepdims=True)
    values = values * lax.rsqrt(mean_square + norm_eps)
    gains = at["mix_gain"][...].astype(jnp.float32)
    normed = jnp.concatenate(
        [
            values[:, k * lanes : (k + 1) * lanes] * gains[k : k + 1]
            for k in range(gains.shape[0])
        ],
        axis=1,
    ).astype(jnp.bfloat16)

    copies["routes"].wait()
    slot_ids = lax.broadcasted_iota(jnp.int32, (slots, seqs), 0)
    picked = jnp.zeros((slots, seqs), jnp.bool_)
    for k in range(at["routes"].shape[0]):
        picked = picked | ((slot_ids >> 2) == at["routes"][k : k + 1])
    earlier = lax.broadcasted_iota(jnp.int32, (seqs, seqs), 0) < lax.broadcasted_iota(
        jnp.int32, (seqs, seqs), 1
    )
    rank = dot32(
        jnp.where(picked, 1.0, 0.0).astype(jnp.bfloat16),
        jnp.where(earlier, 1.0, 0.0).astype(jnp.bfloat16),
    )
    in_slot[...] = jnp.where(
        picked & (rank.astype(jnp.int32) == (slot_ids & 3)), 1.0, 0.0
    )

    raws = []
    for name in ("proj_x", "proj_b", "proj_c"):
        copies[name].wait()
        raws.append(dot32(normed, at[name][...]))
    for name in ("proj_step", "conv_taps", "conv_state", "step_bias", "decay_rate"):
        copies[name].wait()
    conv_state, conv_taps = at["conv_state"], at["conv_taps"]
    parts = []
    for k, raw in enumerate(raws):
        fresh = raw.astype(jnp.bfloat16)
        taps = conv_taps[k].astype(jnp.float32)
        total = fresh.astype(jnp.float32) * taps[3:4]
        for pos in range(3):
            total = total + conv_state[k, pos].astype(jnp.float32) * taps[pos : pos + 1]
        new_conv[k, 0] = conv_state[k, 1]
        new_conv[k, 1] = conv_state[k, 2]
        new_conv[k, 2] = fresh
        parts.append(silu(total))
    conv_copy = pltpu.make_async_copy(new_conv, conv_out, out_sems.at[STATE_CHUNKS])
    conv_copy.start()
    xs, bs, cs = parts
    step_all = lax.dot_general(
        normed, at["proj_step"][...], (((1,), (1,)), ((), ())), preferred_element_type=jnp.float32
    )
    head_ids = lax.broadcasted_iota(jnp.int32, step_all.shape, 1)
    lane_ids = lax.broadcasted_iota(jnp.int32, (seqs, lanes), 1)
    steps, keeps = [], []
    for h in range(heads):
        raw = jnp.sum(
            jnp.where(head_ids == place[0] * heads + h, step_all, 0.0), axis=1, keepdims=True
        )
        raw = raw + at["step_bias"][h]
        step = jnp.maximum(raw, 0.0) + jnp.log1p(jnp.exp(-jnp.abs(raw)))
        steps.append(step)
        keeps.append(jnp.exp(-at["decay_rate"][h] * step))
    driven = xs * jnp.where(lane_ids < head_dim, steps[0], steps[1])
    blank = jnp.zeros((lanes - 3 * seqs, lanes), jnp.float32)
    high, low = in_two(driven)
    columns = jnp.concatenate([high, low, high, blank], axis=0).T
    high, low = in_two(bs)
    b_rows = jnp.concatenate([high, high, low, blank], axis=0).astype(jnp.bfloat16)
    blank = jnp.zeros((lanes - seqs, lanes), jnp.float32)
    c_high, c_low = [
        jnp.concatenate([c, blank], axis=0).astype(jnp.bfloat16) for c in in_two(cs)
    ]
    for h in range(heads):
        keep_rows[h] = jnp.broadcast_to(keeps[h], (seqs, lanes))
    wide_ids = lax.broadcasted_iota(jnp.int32, (heads * head_dim, lanes), 1)
    lots = heads * head_dim
    some = seqs // STATE_CHUNKS

    def chunk(i, read):
        first = pl.multiple_of(i * some, some)
        state_copy(i).wait()
        masked = [
            jnp.where((wide_ids & (seqs - 1)) == first + k, columns, 0.0).astype(jnp.bfloat16)
            for k in range(some)
        ]
        outer = dot32(jnp.concatenate(masked, axis=0), b_rows)
        states = []
        for h in range(heads):
            keep = keep_rows[h, pl.ds(first, some)]
            for k in range(some):
                at_row = k * lots + h * head_dim
                state = (
                    keep[k : k + 1] * scan_state[first + k, h]
                    + outer[at_row : at_row + head_dim]
                )
                new_state[first + k, h] = state
                states.append((at_row, state))
        out_copy(i).start()
        states = jnp.concatenate([state for _, state in sorted(states, key=lambda x: x[0])])
        high, low = [x.astype(jnp.bfloat16) for x in in_two(states)]
        found = across_last(high, c_high) + (across_last(low, c_high) + across_last(high, c_low))
        for k in range(some):
            read = read + jnp.where(
                wide_ids == first + k, found[k * lots : (k + 1) * lots], 0.0
            )
        return read

    read = lax.fori_loop(0, STATE_CHUNKS, chunk, jnp.zeros((lots, lanes), jnp.float32))
    read = read.T[:seqs]
    copies["proj_z"].wait()
    copies["inner_gain"].wait()
    gate = silu(dot32(normed, at["proj_z"][...])) * at["inner_gain"][...].astype(jnp.float32)
    gated = (read * gate).astype(jnp.bfloat16)
    copies["proj_out"].wait()
    part[...] = dot32(gated, at["proj_out"][...]).astype(jnp.bfloat16)
    for i in range(STATE_CHUNKS):
        out_copy(i).wait()
    conv_copy.wait()


def mixer(slots, place, **arrays):
    arrays = [arrays[name] for name in MIXER_INPUTS]
    at = dict(zip(MIXER_INPUTS, arrays))
    resid, conv_state, scan_state = at["resid"], at["conv_state"], at["scan_state"]
    vmem = pl.BlockSpec(memory_space=pltpu.VMEM)
    hbm = pl.BlockSpec(memory_space=pltpu.HBM)
    scalars = ("step_bias", "decay_rate")
    held = [
        (pltpu.SMEM if name in scalars else pltpu.VMEM)(array.shape, array.dtype)
        for name, array in at.items()
    ]
    return pl.pallas_call(
        mixer_kernel,
        name="mixer",
        in_specs=[pl.BlockSpec(memory_space=pltpu.SMEM)] + [hbm] * len(arrays),
        out_specs=[vmem, hbm, hbm, vmem],
        scratch_shapes=held
        + [
            pltpu.VMEM(scan_state.shape, scan_state.dtype),
            pltpu.VMEM(conv_state.shape, conv_state.dtype),
            pltpu.VMEM((scan_state.shape[1], resid.shape[0], scan_state.shape[3]), jnp.float32),
            pltpu.SemaphoreType.DMA((len(arrays),)),
            pltpu.SemaphoreType.DMA((STATE_CHUNKS,)),
            pltpu.SemaphoreType.DMA((STATE_CHUNKS + 1,)),
        ],
        out_shape=[
            jax.ShapeDtypeStruct(resid.shape, jnp.bfloat16),
            jax.ShapeDtypeStruct(scan_state.shape, jnp.float32),
            jax.ShapeDtypeStruct(conv_state.shape, jnp.bfloat16),
            jax.ShapeDtypeStruct((slots, resid.shape[0]), jnp.float32),
        ],
    )(place, *arrays)


def feeder_kernel(
    place, part_0, part_1, part_2, part_3, resid, post_gain, ffn_gain, in_slot,
    stream_quarter, feed, feed_quarter, outgoing,
):
    mixed = sum_of([part_0[...], part_1[...], part_2[...], part_3[...]])
    total = resid[...].astype(jnp.float32) + scaled_rows(mixed, post_gain[...])
    total = total.astype(jnp.bfloat16)
    fed = scaled_rows(total, ffn_gain[...]).astype(jnp.bfloat16)
    feed[...] = fed
    quarter = feed_quarter.shape[1]
    for q in range(feed.shape[1] // quarter):

        @pl.when(place[0] == q)
        def _(q=q):
            stream_quarter[...] = total[:, q * quarter : (q + 1) * quarter]
            feed_quarter[...] = fed[:, q * quarter : (q + 1) * quarter]

    outgoing[...] = dot32(in_slot[...], fed).reshape(outgoing.shape).astype(jnp.bfloat16)


def feeder(quarter, place, *arrays):
    vmem = pl.BlockSpec(memory_space=pltpu.VMEM)
    rows = jax.ShapeDtypeStruct(arrays[0].shape, jnp.bfloat16)
    share = jax.ShapeDtypeStruct((arrays[0].shape[0], quarter), jnp.bfloat16)
    return pl.pallas_call(
        feeder_kernel,
        name="feeder",
        in_specs=[pl.BlockSpec(memory_space=pltpu.SMEM)] + [vmem] * len(arrays),
        out_specs=[vmem] * 4,
        compiler_params=pltpu.CompilerParams(vmem_limit_bytes=FEEDER_VMEM),
        out_shape=[
            share,
            rows,
            share,
            jax.ShapeDtypeStruct((arrays[-1].shape[0] // 4, 4, arrays[0].shape[1]), jnp.bfloat16),
        ],
    )(place, *arrays)


def on_device(
    resid,
    mix_gain,
    proj_x,
    proj_z,
    proj_b,
    proj_c,
    proj_step,
    step_bias,
    decay_rate,
    conv_taps,
    conv_state,
    scan_state,
    inner_gain,
    proj_out,
    post_gain,
    ffn_gain,
    group_router,
    expert_router,
    route_experts,
    expert_gate,
    expert_up,
    expert_down,
    dense_switch,
    dense_gate,
    dense_up,
    dense_down,
    out_gain,
):
    tp_index = lax.axis_index("tp")
    tp_count = lax.axis_size("tp")
    seqs, width = resid.shape
    quarter = width // tp_count
    channels = conv_state.shape[3]
    units = dense_gate.shape[0]

    blocks = jnp.stack([dense_gate, dense_up, dense_down])[None]
    blocks = jnp.concatenate([blocks, from_flip(blocks, "ep_0", 4)])
    blocks = jnp.concatenate([blocks, from_flip(blocks, "ep_0", 2)])
    blocks = jnp.concatenate([blocks, from_flip(blocks, "ep_0", 1)])
    unit_rows = jnp.moveaxis(blocks, 0, 1).reshape(3, blocks.shape[0] * units, quarter)
    expert_count = expert_router.shape[1]
    group_size = expert_count // group_router.shape[1]
    pick_count = route_experts.shape[1]
    capacity = 2 * seqs * pick_count // expert_count

    place = jnp.full((1,), tp_index, jnp.int32)
    part, new_state, new_conv, in_slot = mixer(
        expert_count * capacity,
        place,
        resid=resid,
        mix_gain=mix_gain.reshape(-1, channels),
        routes=route_experts.T,
        proj_x=proj_x,
        proj_b=proj_b,
        proj_c=proj_c,
        proj_step=proj_step.T,
        conv_taps=conv_taps,
        conv_state=conv_state.transpose(1, 2, 0, 3),
        step_bias=step_bias,
        decay_rate=decay_rate,
        scan_state=scan_state,
        proj_z=proj_z,
        inner_gain=inner_gain[None],
        proj_out=proj_out,
    )
    new_conv = new_conv.transpose(2, 0, 1, 3)
    mixed_parts = from_all(part, "tp")
    mixed_parts[0] = part.astype(jnp.float32)
    down, part = lax.optimization_barrier((expert_down[0], part))
    down_parts = [
        lax.dynamic_slice_in_dim(down, ((tp_index + s) % tp_count) * quarter, quarter, 1)
        for s in range(tp_count)
    ]
    stream_quarter, feed, feed_quarter, outgoing = feeder(
        quarter, place, *mixed_parts, resid.astype(jnp.float32), post_gain[None],
        ffn_gain[None], in_slot.astype(jnp.bfloat16),
    )

    arrived = lax.all_to_all(
        outgoing, EP, 0, 0, tiled=True
    )
    rows = arrived.reshape(expert_count * capacity, width)

    tokens = jnp.concatenate([feed_quarter, from_flip(feed_quarter, "ep_2", 1)], axis=0)
    tokens = jnp.concatenate(from_all(tokens, "ep_1"), axis=0)
    feed, tokens = lax.optimization_barrier((feed, tokens))
    gate_rows, up_rows, down_rows = unit_rows
    down_parts = [down_parts[0]] + [from_shift(down_parts[s], "tp", s) for s in range(1, tp_count)]
    across = (((1,), (1,)), ((), ()))
    gate_piece = lax.dot_general(tokens, gate_rows, across, preferred_element_type=jnp.float32)
    up_piece = lax.dot_general(tokens, up_rows, across, preferred_element_type=jnp.float32)
    pieces = jnp.stack([gate_piece, up_piece]).astype(jnp.bfloat16)
    sums = from_all(pieces, "tp")

    gate_value = dot32(rows, expert_gate[0])
    up_value = dot32(rows, expert_up[0])
    hidden = (jax.nn.silu(gate_value) * up_value).astype(jnp.bfloat16)
    _, *sums = lax.optimization_barrier((hidden, *sums))
    hidden_parts = from_all(hidden, "tp")
    sums = sum_of(sums)
    dense_hidden = (jax.nn.silu(sums[0]) * sums[1]).astype(jnp.bfloat16)
    dense_part = dot32(dense_hidden, down_rows).astype(jnp.bfloat16)
    lots = dense_part.reshape(lax.axis_size("ep_1"), 2 * seqs, quarter)
    lots = sum_of([lots[0]] + [from_shift(lots[b], "ep_1", -b) for b in range(1, lots.shape[0])])
    dense_part = lots[:seqs] + from_flip(lots[seqs:].astype(jnp.bfloat16), "ep_2", 1)
    dense_out = dense_part

    served = dot32(
        jnp.concatenate(hidden_parts, axis=1), jnp.concatenate(down_parts, axis=0)
    ).astype(jnp.bfloat16)
    returned = lax.all_to_all(
        served.reshape(expert_count, capacity, quarter), EP, 0, 0, tiled=True
    ).reshape(expert_count * capacity, quarter)

    features = (((0,), (1,)), ((), ()))
    group_exp = jnp.exp(
        lax.dot_general(group_router, feed, features, preferred_element_type=jnp.float32)
    )
    group_prob = group_exp / jnp.sum(group_exp, axis=0, keepdims=True)
    routes = route_experts.T
    group_ids = jnp.arange(group_router.shape[1], dtype=jnp.int32)[:, None]
    group_weight = jnp.sum(
        jnp.where(routes[:1] // group_size == group_ids, group_prob, 0.0), axis=0, keepdims=True
    )
    expert_ids = jnp.arange(expert_count, dtype=jnp.int32)[:, None]
    picked = expert_ids == routes[0:1]
    for k in range(1, pick_count):
        picked = picked | (expert_ids == routes[k : k + 1])
    logits = lax.dot_general(expert_router, feed, features, preferred_element_type=jnp.float32)
    pick_exp = jnp.exp(jnp.where(picked, logits, -jnp.inf))
    pick_weight = pick_exp / jnp.sum(pick_exp, axis=0, keepdims=True) * group_weight
    slot_weight = in_slot * jnp.repeat(pick_weight, capacity, axis=0)
    weight_high = slot_weight.astype(jnp.bfloat16)
    weight_low = (slot_weight - weight_high.astype(jnp.float32)).astype(jnp.bfloat16)
    slotwise = (((0,), (0,)), ((), ()))
    routed = lax.dot_general(
        weight_high, returned, slotwise, preferred_element_type=jnp.float32
    ) + lax.dot_general(weight_low, returned, slotwise, preferred_element_type=jnp.float32)

    switch = jax.nn.sigmoid(dot32(feed, dense_switch))
    combined = routed + switch[:, None] * dense_out
    squares = jnp.sum(combined * combined, axis=1)
    total_square = sum_of(from_all(squares, "tp"))
    scale = lax.rsqrt(total_square / width + norm_eps)
    layer_out = (stream_quarter.astype(jnp.float32) + combined * scale[:, None] * out_gain.astype(jnp.float32)).astype(
        jnp.bfloat16
    )
    return (layer_out, new_state, new_conv)


def solution(mesh):
    torus = Mesh(mesh.devices.reshape(8, 4, 2, mesh.shape["tp"]), ("ep_0", "ep_1", "ep_2", "tp"))
    in_specs = (
        P(EP, None),
        P(),
        P(None, "tp"),
        P(None, "tp"),
        P(None, "tp"),
        P(None, "tp"),
        P(),
        P("tp"),
        P("tp"),
        P(None, None, "tp"),
        P(EP, None, None, "tp"),
        P(EP, "tp", None, None),
        P("tp"),
        P("tp", None),
        P(),
        P(),
        P(),
        P(),
        P(EP, None),
        P(EP, None, "tp"),
        P(EP, None, "tp"),
        P(EP, "tp", None),
        P(),
        P(EP, "tp"),
        P(EP, "tp"),
        P(EP, "tp"),
        P("tp"),
    )
    out_specs = (P(EP, "tp"), P(EP, "tp", None, None), P(EP, None, None, "tp"))

    return jax.shard_map(
        on_device, mesh=torus, in_specs=in_specs, out_specs=out_specs, check_vma=False
    )
```

```python
import jax
import jax.numpy as jnp
from jax import lax
from jax.sharding import Mesh
from jax.experimental import pallas as pl
from jax.experimental.pallas import tpu as pltpu
from jax.sharding import PartitionSpec as P


EP = ("ep_0", "ep_1", "ep_2")


norm_eps = 1e-06
FEEDER_VMEM = 16 * 2**20
STATE_CHUNKS = 4


def from_shift(array, axis, shift):
    count = lax.axis_size(axis)
    return lax.ppermute(array, axis, [(i, (i + shift) % count) for i in range(count)])


def from_all(array, axis):
    count = lax.axis_size(axis)
    return [array] + [from_shift(array, axis, s) for s in range(1, count)]


def scaled_rows(values, gain):
    values = values.astype(jnp.float32)
    mean_square = jnp.mean(values * values, axis=-1, keepdims=True)
    return values * lax.rsqrt(mean_square + norm_eps) * gain.astype(jnp.float32)


def dot32(a, b):
    return jnp.dot(a, b, preferred_element_type=jnp.float32)


def sum_of(arrays):
    total = arrays[0].astype(jnp.float32)
    for array in arrays[1:]:
        total = total + array.astype(jnp.float32)
    return total


def from_flip(array, axis, bit):
    count = lax.axis_size(axis)
    return lax.ppermute(array, axis, [(i, i ^ bit) for i in range(count)])


def silu(values):
    return values * (1.0 / (1.0 + jnp.exp(-values)))


MIXER_INPUTS = (
    "resid", "mix_gain", "proj_x", "proj_b", "proj_c", "proj_step", "conv_taps",
    "conv_state", "step_bias", "decay_rate", "scan_state", "proj_z", "inner_gain", "proj_out",
)


def in_two(values):
    high = values.astype(jnp.bfloat16).astype(jnp.float32)
    return high, values - high


def across_last(a, b):
    return lax.dot_general(a, b, (((1,), (1,)), ((), ())), preferred_element_type=jnp.float32)


def mixer_kernel(place, *refs):
    count = len(MIXER_INPUTS)
    sources, refs = refs[:count], refs[count:]
    (part, state_out, conv_out), refs = refs[:3], refs[3:]
    held, refs = refs[:count], refs[count:]
    new_state, new_conv, keep_rows, sems, in_sems, out_sems = refs
    at = dict(zip(MIXER_INPUTS, held))
    scan_state = at["scan_state"]
    copies = {
        name: pltpu.make_async_copy(source, target, sems.at[k])
        for k, (name, source, target) in enumerate(zip(MIXER_INPUTS, sources, held))
        if name != "scan_state"
    }
    state_in = dict(zip(MIXER_INPUTS, sources))["scan_state"]

    def share(i):
        some = state_in.shape[0] // STATE_CHUNKS
        return pl.ds(i * some, some)

    def state_copy(i):
        return pltpu.make_async_copy(
            state_in.at[share(i)], scan_state.at[share(i)], in_sems.at[i]
        )

    def out_copy(i):
        return pltpu.make_async_copy(
            new_state.at[share(i)], state_out.at[share(i)], out_sems.at[i]
        )

    for name in MIXER_INPUTS:
        if name == "scan_state":
            for i in range(STATE_CHUNKS):
                state_copy(i).start()
        else:
            copies[name].start()

    seqs = part.shape[0]
    heads, head_dim, lanes = new_state.shape[1:]
    copies["resid"].wait()
    copies["mix_gain"].wait()
    values = at["resid"][...].astype(jnp.float32)
    mean_square = jnp.mean(values * values, axis=-1, keepdims=True)
    values = values * lax.rsqrt(mean_square + norm_eps)
    gains = at["mix_gain"][...].astype(jnp.float32)
    normed = jnp.concatenate(
        [
            values[:, k * lanes : (k + 1) * lanes] * gains[k : k + 1]
            for k in range(gains.shape[0])
        ],
        axis=1,
    ).astype(jnp.bfloat16)

    raws = []
    for name in ("proj_x", "proj_b", "proj_c"):
        copies[name].wait()
        raws.append(dot32(normed, at[name][...]))
    for name in ("proj_step", "conv_taps", "conv_state", "step_bias", "decay_rate"):
        copies[name].wait()
    conv_state, conv_taps = at["conv_state"], at["conv_taps"]
    parts = []
    for k, raw in enumerate(raws):
        fresh = raw.astype(jnp.bfloat16)
        taps = conv_taps[k].astype(jnp.float32)
        total = fresh.astype(jnp.float32) * taps[3:4]
        for pos in range(3):
            total = total + conv_state[k, pos].astype(jnp.float32) * taps[pos : pos + 1]
        new_conv[k, 0] = conv_state[k, 1]
        new_conv[k, 1] = conv_state[k, 2]
        new_conv[k, 2] = fresh
        parts.append(silu(total))
    conv_copy = pltpu.make_async_copy(new_conv, conv_out, out_sems.at[STATE_CHUNKS])
    conv_copy.start()
    xs, bs, cs = parts
    step_all = lax.dot_general(
        normed, at["proj_step"][...], (((1,), (1,)), ((), ())), preferred_element_type=jnp.float32
    )
    head_ids = lax.broadcasted_iota(jnp.int32, step_all.shape, 1)
    lane_ids = lax.broadcasted_iota(jnp.int32, (seqs, lanes), 1)
    steps, keeps = [], []
    for h in range(heads):
        raw = jnp.sum(
            jnp.where(head_ids == place[0] * heads + h, step_all, 0.0), axis=1, keepdims=True
        )
        raw = raw + at["step_bias"][h]
        step = jnp.maximum(raw, 0.0) + jnp.log1p(jnp.exp(-jnp.abs(raw)))
        steps.append(step)
        keeps.append(jnp.exp(-at["decay_rate"][h] * step))
    driven = xs * jnp.where(lane_ids < head_dim, steps[0], steps[1])
    blank = jnp.zeros((lanes - 3 * seqs, lanes), jnp.float32)
    high, low = in_two(driven)
    columns = jnp.concatenate([high, low, high, blank], axis=0).T
    high, low = in_two(bs)
    b_rows = jnp.concatenate([high, high, low, blank], axis=0).astype(jnp.bfloat16)
    blank = jnp.zeros((lanes - seqs, lanes), jnp.float32)
    c_high, c_low = [
        jnp.concatenate([c, blank], axis=0).astype(jnp.bfloat16) for c in in_two(cs)
    ]
    for h in range(heads):
        keep_rows[h] = jnp.broadcast_to(keeps[h], (seqs, lanes))
    wide_ids = lax.broadcasted_iota(jnp.int32, (heads * head_dim, lanes), 1)
    lots = heads * head_dim
    some = seqs // STATE_CHUNKS

    def chunk(i, read):
        first = pl.multiple_of(i * some, some)
        state_copy(i).wait()
        masked = [
            jnp.where((wide_ids & (seqs - 1)) == first + k, columns, 0.0).astype(jnp.bfloat16)
            for k in range(some)
        ]
        outer = dot32(jnp.concatenate(masked, axis=0), b_rows)
        states = []
        for h in range(heads):
            keep = keep_rows[h, pl.ds(first, some)]
            for k in range(some):
                at_row = k * lots + h * head_dim
                state = (
                    keep[k : k + 1] * scan_state[first + k, h]
                    + outer[at_row : at_row + head_dim]
                )
                new_state[first + k, h] = state
                states.append((at_row, state))
        out_copy(i).start()
        states = jnp.concatenate([state for _, state in sorted(states, key=lambda x: x[0])])
        high, low = [x.astype(jnp.bfloat16) for x in in_two(states)]
        found = across_last(high, c_high) + (across_last(low, c_high) + across_last(high, c_low))
        for k in range(some):
            read = read + jnp.where(
                wide_ids == first + k, found[k * lots : (k + 1) * lots], 0.0
            )
        return read

    read = lax.fori_loop(0, STATE_CHUNKS, chunk, jnp.zeros((lots, lanes), jnp.float32))
    read = read.T[:seqs]
    copies["proj_z"].wait()
    copies["inner_gain"].wait()
    gate = silu(dot32(normed, at["proj_z"][...])) * at["inner_gain"][...].astype(jnp.float32)
    gated = (read * gate).astype(jnp.bfloat16)
    copies["proj_out"].wait()
    part[...] = dot32(gated, at["proj_out"][...]).astype(jnp.bfloat16)
    for i in range(STATE_CHUNKS):
        out_copy(i).wait()
    conv_copy.wait()


def mixer(place, **arrays):
    arrays = [arrays[name] for name in MIXER_INPUTS]
    at = dict(zip(MIXER_INPUTS, arrays))
    resid, conv_state, scan_state = at["resid"], at["conv_state"], at["scan_state"]
    vmem = pl.BlockSpec(memory_space=pltpu.VMEM)
    hbm = pl.BlockSpec(memory_space=pltpu.HBM)
    scalars = ("step_bias", "decay_rate")
    held = [
        (pltpu.SMEM if name in scalars else pltpu.VMEM)(array.shape, array.dtype)
        for name, array in at.items()
    ]
    return pl.pallas_call(
        mixer_kernel,
        name="mixer",
        in_specs=[pl.BlockSpec(memory_space=pltpu.SMEM)] + [hbm] * len(arrays),
        out_specs=[vmem, hbm, hbm],
        scratch_shapes=held
        + [
            pltpu.VMEM(scan_state.shape, scan_state.dtype),
            pltpu.VMEM(conv_state.shape, conv_state.dtype),
            pltpu.VMEM((scan_state.shape[1], resid.shape[0], scan_state.shape[3]), jnp.float32),
            pltpu.SemaphoreType.DMA((len(arrays),)),
            pltpu.SemaphoreType.DMA((STATE_CHUNKS,)),
            pltpu.SemaphoreType.DMA((STATE_CHUNKS + 1,)),
        ],
        out_shape=[
            jax.ShapeDtypeStruct(resid.shape, jnp.bfloat16),
            jax.ShapeDtypeStruct(scan_state.shape, jnp.float32),
            jax.ShapeDtypeStruct(conv_state.shape, jnp.bfloat16),
        ],
    )(place, *arrays)


def expert_in_kernel(rows, gate, up, hidden):
    gate_value = dot32(rows[...], gate[...])
    hidden[...] = (silu(gate_value) * dot32(rows[...], up[...])).astype(jnp.bfloat16)


def expert_out_kernel(*refs):
    half = len(refs) // 2
    total = dot32(refs[0][...], refs[half][...])
    for k in range(1, half):
        total = total + dot32(refs[k][...], refs[half + k][...])
    refs[-1][...] = total.astype(jnp.bfloat16)


def simple_call(kernel, shape, *arrays):
    vmem = pl.BlockSpec(memory_space=pltpu.VMEM)
    return pl.pallas_call(
        kernel,
        in_specs=[vmem] * len(arrays),
        out_specs=vmem,
        compiler_params=pltpu.CompilerParams(vmem_limit_bytes=FEEDER_VMEM),
        out_shape=jax.ShapeDtypeStruct(shape, jnp.bfloat16),
    )(*arrays)


def feeder_kernel(
    place, part_0, part_1, part_2, part_3, resid, post_gain, ffn_gain, routes,
    stream_quarter, feed, feed_quarter, outgoing, in_slot,
):
    slots, seqs = in_slot.shape
    slot_ids = lax.broadcasted_iota(jnp.int32, (slots, seqs), 0)
    picked = jnp.zeros((slots, seqs), jnp.bool_)
    for k in range(routes.shape[0]):
        picked = picked | ((slot_ids >> 2) == routes[k : k + 1])
    earlier = lax.broadcasted_iota(jnp.int32, (seqs, seqs), 0) < lax.broadcasted_iota(
        jnp.int32, (seqs, seqs), 1
    )
    rank = dot32(
        jnp.where(picked, 1.0, 0.0).astype(jnp.bfloat16),
        jnp.where(earlier, 1.0, 0.0).astype(jnp.bfloat16),
    )
    placed = jnp.where(picked & (rank.astype(jnp.int32) == (slot_ids & 3)), 1.0, 0.0)
    in_slot[...] = placed
    mixed = sum_of([part_0[...], part_1[...], part_2[...], part_3[...]])
    total = resid[...].astype(jnp.float32) + scaled_rows(mixed, post_gain[...])
    total = total.astype(jnp.bfloat16)
    fed = scaled_rows(total, ffn_gain[...]).astype(jnp.bfloat16)
    feed[...] = fed
    quarter = feed_quarter.shape[1]
    for q in range(feed.shape[1] // quarter):

        @pl.when(place[0] == q)
        def _(q=q):
            stream_quarter[...] = total[:, q * quarter : (q + 1) * quarter]
            feed_quarter[...] = fed[:, q * quarter : (q + 1) * quarter]

    outgoing[...] = dot32(placed.astype(jnp.bfloat16), fed).reshape(outgoing.shape).astype(jnp.bfloat16)


def feeder(slots, quarter, place, *arrays):
    vmem = pl.BlockSpec(memory_space=pltpu.VMEM)
    rows = jax.ShapeDtypeStruct(arrays[0].shape, jnp.bfloat16)
    share = jax.ShapeDtypeStruct((arrays[0].shape[0], quarter), jnp.bfloat16)
    return pl.pallas_call(
        feeder_kernel,
        name="feeder",
        in_specs=[pl.BlockSpec(memory_space=pltpu.SMEM)] + [vmem] * len(arrays),
        out_specs=[vmem] * 5,
        compiler_params=pltpu.CompilerParams(vmem_limit_bytes=FEEDER_VMEM),
        out_shape=[
            share,
            rows,
            share,
            jax.ShapeDtypeStruct((slots // 4, 4, arrays[0].shape[1]), jnp.bfloat16),
            jax.ShapeDtypeStruct((slots, arrays[0].shape[0]), jnp.float32),
        ],
    )(place, *arrays)


def on_device(
    resid,
    mix_gain,
    proj_x,
    proj_z,
    proj_b,
    proj_c,
    proj_step,
    step_bias,
    decay_rate,
    conv_taps,
    conv_state,
    scan_state,
    inner_gain,
    proj_out,
    post_gain,
    ffn_gain,
    group_router,
    expert_router,
    route_experts,
    expert_gate,
    expert_up,
    expert_down,
    dense_switch,
    dense_gate,
    dense_up,
    dense_down,
    out_gain,
):
    tp_index = lax.axis_index("tp")
    tp_count = lax.axis_size("tp")
    seqs, width = resid.shape
    quarter = width // tp_count
    channels = conv_state.shape[3]
    units = dense_gate.shape[0]

    blocks = jnp.stack([dense_gate, dense_up, dense_down])[None]
    blocks = jnp.concatenate([blocks, from_flip(blocks, "ep_0", 4)])
    blocks = jnp.concatenate([blocks, from_flip(blocks, "ep_0", 2)])
    unit_rows = jnp.moveaxis(blocks, 0, 1).reshape(3, blocks.shape[0] * units, quarter)
    expert_count = expert_router.shape[1]
    group_size = expert_count // group_router.shape[1]
    pick_count = route_experts.shape[1]
    capacity = 2 * seqs * pick_count // expert_count

    place = jnp.full((1,), tp_index, jnp.int32)
    part, new_state, new_conv = mixer(
        place,
        resid=resid,
        mix_gain=mix_gain.reshape(-1, channels),
        proj_x=proj_x,
        proj_b=proj_b,
        proj_c=proj_c,
        proj_step=proj_step.T,
        conv_taps=conv_taps,
        conv_state=conv_state.transpose(1, 2, 0, 3),
        step_bias=step_bias,
        decay_rate=decay_rate,
        scan_state=scan_state,
        proj_z=proj_z,
        inner_gain=inner_gain[None],
        proj_out=proj_out,
    )
    new_conv = new_conv.transpose(2, 0, 1, 3)
    mixed_parts = from_all(part, "tp")
    mixed_parts[0] = part.astype(jnp.float32)
    stream_quarter, feed, feed_quarter, outgoing, in_slot = feeder(
        expert_count * capacity, quarter, place, *mixed_parts, resid.astype(jnp.float32),
        post_gain[None], ffn_gain[None], route_experts.T,
    )

    arrived = lax.all_to_all(
        outgoing, EP, 0, 0, tiled=True
    )
    rows = arrived.reshape(expert_count * capacity, width)

    tokens = jnp.concatenate([feed_quarter, from_flip(feed_quarter, "ep_0", 1)], axis=0)
    tokens = jnp.concatenate(from_all(tokens, "ep_1"), axis=0)
    tokens = jnp.concatenate([tokens, from_flip(tokens, "ep_2", 1)], axis=0)
    feed, tokens = lax.optimization_barrier((feed, tokens))
    gate_rows, up_rows, down_rows = unit_rows
    down = expert_down[0]
    down_parts = [
        lax.dynamic_slice_in_dim(down, ((tp_index + s) % tp_count) * quarter, quarter, 1)
        for s in range(tp_count)
    ]
    down_parts = [down_parts[0]] + [from_shift(down_parts[s], "tp", s) for s in range(1, tp_count)]
    across = (((1,), (1,)), ((), ()))
    gate_piece = lax.dot_general(tokens, gate_rows, across, preferred_element_type=jnp.float32)
    up_piece = lax.dot_general(tokens, up_rows, across, preferred_element_type=jnp.float32)
    pieces = jnp.stack([gate_piece, up_piece]).astype(jnp.bfloat16)
    sums = from_all(pieces, "tp")

    features = (((0,), (1,)), ((), ()))
    group_exp = jnp.exp(
        lax.dot_general(group_router, feed, features, preferred_element_type=jnp.float32)
    )
    group_prob = group_exp / jnp.sum(group_exp, axis=0, keepdims=True)
    routes = route_experts.T
    group_ids = jnp.arange(group_router.shape[1], dtype=jnp.int32)[:, None]
    group_weight = jnp.sum(
        jnp.where(routes[:1] // group_size == group_ids, group_prob, 0.0), axis=0, keepdims=True
    )
    expert_ids = jnp.arange(expert_count, dtype=jnp.int32)[:, None]
    picked = expert_ids == routes[0:1]
    for k in range(1, pick_count):
        picked = picked | (expert_ids == routes[k : k + 1])
    logits = lax.dot_general(expert_router, feed, features, preferred_element_type=jnp.float32)
    pick_exp = jnp.exp(jnp.where(picked, logits, -jnp.inf))
    pick_weight = pick_exp / jnp.sum(pick_exp, axis=0, keepdims=True) * group_weight
    slot_weight = in_slot * jnp.repeat(pick_weight, capacity, axis=0)
    weight_high = slot_weight.astype(jnp.bfloat16)
    weight_low = (slot_weight - weight_high.astype(jnp.float32)).astype(jnp.bfloat16)
    switch = jax.nn.sigmoid(dot32(feed, dense_switch))
    rows, weight_high, weight_low, switch = lax.optimization_barrier(
        (rows, weight_high, weight_low, switch)
    )

    hidden = simple_call(
        expert_in_kernel, (rows.shape[0], expert_gate.shape[2]),
        rows, expert_gate[0], expert_up[0],
    )
    _, *sums = lax.optimization_barrier((hidden, *sums))
    hidden_parts = from_all(hidden, "tp")
    sums = sum_of(sums)
    dense_hidden = (jax.nn.silu(sums[0]) * sums[1]).astype(jnp.bfloat16)
    dense_part = dot32(dense_hidden, down_rows).astype(jnp.bfloat16)
    half = dense_part.shape[0] // 2
    lots = sum_of([dense_part[:half], from_flip(dense_part[half:], "ep_2", 1)])
    lots = lots.astype(jnp.bfloat16).reshape(lax.axis_size("ep_1"), 2, seqs, quarter)
    lots = sum_of([lots[:, 0], from_flip(lots[:, 1], "ep_0", 1)])
    lots = lots.astype(jnp.bfloat16)
    dense_part = sum_of(
        [lots[0]] + [from_shift(lots[b], "ep_1", -b) for b in range(1, lots.shape[0])]
    )
    dense_out = dense_part

    served = simple_call(expert_out_kernel, (rows.shape[0], quarter), *hidden_parts, *down_parts)
    returned = lax.all_to_all(
        served.reshape(expert_count, capacity, quarter), EP, 0, 0, tiled=True
    ).reshape(expert_count * capacity, quarter)

    slotwise = (((0,), (0,)), ((), ()))
    routed = lax.dot_general(
        weight_high, returned, slotwise, preferred_element_type=jnp.float32
    ) + lax.dot_general(weight_low, returned, slotwise, preferred_element_type=jnp.float32)

    combined = routed + switch[:, None] * dense_out
    squares = jnp.sum(combined * combined, axis=1)
    total_square = sum_of(from_all(squares, "tp"))
    scale = lax.rsqrt(total_square / width + norm_eps)
    layer_out = (stream_quarter.astype(jnp.float32) + combined * scale[:, None] * out_gain.astype(jnp.float32)).astype(
        jnp.bfloat16
    )
    return (layer_out, new_state, new_conv)


def solution(mesh):
    torus = Mesh(mesh.devices.reshape(8, 4, 2, mesh.shape["tp"]), ("ep_0", "ep_1", "ep_2", "tp"))
    in_specs = (
        P(EP, None),
        P(),
        P(None, "tp"),
        P(None, "tp"),
        P(None, "tp"),
        P(None, "tp"),
        P(),
        P("tp"),
        P("tp"),
        P(None, None, "tp"),
        P(EP, None, None, "tp"),
        P(EP, "tp", None, None),
        P("tp"),
        P("tp", None),
        P(),
        P(),
        P(),
        P(),
        P(EP, None),
        P(EP, None, "tp"),
        P(EP, None, "tp"),
        P(EP, "tp", None),
        P(),
        P(EP, "tp"),
        P(EP, "tp"),
        P(EP, "tp"),
        P("tp"),
    )
    out_specs = (P(EP, "tp"), P(EP, "tp", None, None), P(EP, None, None, "tp"))

    return jax.shard_map(
        on_device, mesh=torus, in_specs=in_specs, out_specs=out_specs, check_vma=False
    )
```

```python
import jax
import jax.numpy as jnp
from jax import lax
from jax.sharding import Mesh
from jax.experimental import pallas as pl
from jax.experimental.pallas import tpu as pltpu
from jax.sharding import PartitionSpec as P


EP = ("ep_0", "ep_1", "ep_2")


norm_eps = 1e-06
FEEDER_VMEM = 16 * 2**20
STATE_CHUNKS = 4
ROW_CHUNKS = 4


def from_shift(array, axis, shift):
    count = lax.axis_size(axis)
    return lax.ppermute(array, axis, [(i, (i + shift) % count) for i in range(count)])


def from_all(array, axis):
    count = lax.axis_size(axis)
    return [array] + [from_shift(array, axis, s) for s in range(1, count)]


def scaled_rows(values, gain):
    values = values.astype(jnp.float32)
    mean_square = jnp.mean(values * values, axis=-1, keepdims=True)
    return values * lax.rsqrt(mean_square + norm_eps) * gain.astype(jnp.float32)


def dot32(a, b):
    return jnp.dot(a, b, preferred_element_type=jnp.float32)


def sum_of(arrays):
    total = arrays[0].astype(jnp.float32)
    for array in arrays[1:]:
        total = total + array.astype(jnp.float32)
    return total


def from_flip(array, axis, bit):
    count = lax.axis_size(axis)
    return lax.ppermute(array, axis, [(i, i ^ bit) for i in range(count)])


def silu(values):
    return values * (1.0 / (1.0 + jnp.exp(-values)))


MIXER_INPUTS = (
    "resid", "mix_gain", "proj_x", "proj_b", "proj_c", "proj_step", "conv_taps",
    "conv_state", "step_bias", "decay_rate", "scan_state", "proj_z", "inner_gain", "proj_out",
)


def in_two(values):
    high = values.astype(jnp.bfloat16).astype(jnp.float32)
    return high, values - high


def across_last(a, b):
    return lax.dot_general(a, b, (((1,), (1,)), ((), ())), preferred_element_type=jnp.float32)


def mixer_kernel(place, *refs):
    count = len(MIXER_INPUTS)
    sources, refs = refs[:count], refs[count:]
    (part, state_out, conv_out), refs = refs[:3], refs[3:]
    held, refs = refs[:count], refs[count:]
    new_state, new_conv, keep_rows, sems, in_sems, out_sems = refs
    at = dict(zip(MIXER_INPUTS, held))
    scan_state = at["scan_state"]
    copies = {
        name: pltpu.make_async_copy(source, target, sems.at[k])
        for k, (name, source, target) in enumerate(zip(MIXER_INPUTS, sources, held))
        if name != "scan_state"
    }
    state_in = dict(zip(MIXER_INPUTS, sources))["scan_state"]

    def share(i):
        some = state_in.shape[0] // STATE_CHUNKS
        return pl.ds(i * some, some)

    def state_copy(i):
        return pltpu.make_async_copy(
            state_in.at[share(i)], scan_state.at[share(i)], in_sems.at[i]
        )

    def out_copy(i):
        return pltpu.make_async_copy(
            new_state.at[share(i)], state_out.at[share(i)], out_sems.at[i]
        )

    for name in MIXER_INPUTS:
        if name == "scan_state":
            for i in range(STATE_CHUNKS):
                state_copy(i).start()
        else:
            copies[name].start()

    seqs = part.shape[0]
    heads, head_dim, lanes = new_state.shape[1:]
    copies["resid"].wait()
    copies["mix_gain"].wait()
    values = at["resid"][...].astype(jnp.float32)
    mean_square = jnp.mean(values * values, axis=-1, keepdims=True)
    values = values * lax.rsqrt(mean_square + norm_eps)
    gains = at["mix_gain"][...].astype(jnp.float32)
    normed = jnp.concatenate(
        [
            values[:, k * lanes : (k + 1) * lanes] * gains[k : k + 1]
            for k in range(gains.shape[0])
        ],
        axis=1,
    ).astype(jnp.bfloat16)

    raws = []
    for name in ("proj_x", "proj_b", "proj_c"):
        copies[name].wait()
        raws.append(dot32(normed, at[name][...]))
    for name in ("proj_step", "conv_taps", "conv_state", "step_bias", "decay_rate"):
        copies[name].wait()
    conv_state, conv_taps = at["conv_state"], at["conv_taps"]
    parts = []
    for k, raw in enumerate(raws):
        fresh = raw.astype(jnp.bfloat16)
        taps = conv_taps[k].astype(jnp.float32)
        total = fresh.astype(jnp.float32) * taps[3:4]
        for pos in range(3):
            total = total + conv_state[k, pos].astype(jnp.float32) * taps[pos : pos + 1]
        new_conv[k, 0] = conv_state[k, 1]
        new_conv[k, 1] = conv_state[k, 2]
        new_conv[k, 2] = fresh
        parts.append(silu(total))
    conv_copy = pltpu.make_async_copy(new_conv, conv_out, out_sems.at[STATE_CHUNKS])
    conv_copy.start()
    xs, bs, cs = parts
    step_all = lax.dot_general(
        normed, at["proj_step"][...], (((1,), (1,)), ((), ())), preferred_element_type=jnp.float32
    )
    head_ids = lax.broadcasted_iota(jnp.int32, step_all.shape, 1)
    lane_ids = lax.broadcasted_iota(jnp.int32, (seqs, lanes), 1)
    steps, keeps = [], []
    for h in range(heads):
        raw = jnp.sum(
            jnp.where(head_ids == place[0] * heads + h, step_all, 0.0), axis=1, keepdims=True
        )
        raw = raw + at["step_bias"][h]
        step = jnp.maximum(raw, 0.0) + jnp.log1p(jnp.exp(-jnp.abs(raw)))
        steps.append(step)
        keeps.append(jnp.exp(-at["decay_rate"][h] * step))
    driven = xs * jnp.where(lane_ids < head_dim, steps[0], steps[1])
    blank = jnp.zeros((lanes - 3 * seqs, lanes), jnp.float32)
    high, low = in_two(driven)
    columns = jnp.concatenate([high, low, high, blank], axis=0).T
    high, low = in_two(bs)
    b_rows = jnp.concatenate([high, high, low, blank], axis=0).astype(jnp.bfloat16)
    blank = jnp.zeros((lanes - seqs, lanes), jnp.float32)
    c_high, c_low = [
        jnp.concatenate([c, blank], axis=0).astype(jnp.bfloat16) for c in in_two(cs)
    ]
    for h in range(heads):
        keep_rows[h] = jnp.broadcast_to(keeps[h], (seqs, lanes))
    wide_ids = lax.broadcasted_iota(jnp.int32, (heads * head_dim, lanes), 1)
    lots = heads * head_dim
    some = seqs // STATE_CHUNKS

    def chunk(i, read):
        first = pl.multiple_of(i * some, some)
        state_copy(i).wait()
        masked = [
            jnp.where((wide_ids & (seqs - 1)) == first + k, columns, 0.0).astype(jnp.bfloat16)
            for k in range(some)
        ]
        outer = dot32(jnp.concatenate(masked, axis=0), b_rows)
        states = []
        for h in range(heads):
            keep = keep_rows[h, pl.ds(first, some)]
            for k in range(some):
                at_row = k * lots + h * head_dim
                state = (
                    keep[k : k + 1] * scan_state[first + k, h]
                    + outer[at_row : at_row + head_dim]
                )
                new_state[first + k, h] = state
                states.append((at_row, state))
        out_copy(i).start()
        states = jnp.concatenate([state for _, state in sorted(states, key=lambda x: x[0])])
        high, low = [x.astype(jnp.bfloat16) for x in in_two(states)]
        found = across_last(high, c_high) + (across_last(low, c_high) + across_last(high, c_low))
        for k in range(some):
            read = read + jnp.where(
                wide_ids == first + k, found[k * lots : (k + 1) * lots], 0.0
            )
        return read

    read = lax.fori_loop(0, STATE_CHUNKS, chunk, jnp.zeros((lots, lanes), jnp.float32))
    read = read.T[:seqs]
    copies["proj_z"].wait()
    copies["inner_gain"].wait()
    gate = silu(dot32(normed, at["proj_z"][...])) * at["inner_gain"][...].astype(jnp.float32)
    gated = (read * gate).astype(jnp.bfloat16)
    copies["proj_out"].wait()
    part[...] = dot32(gated, at["proj_out"][...]).astype(jnp.bfloat16)
    for i in range(STATE_CHUNKS):
        out_copy(i).wait()
    conv_copy.wait()


def mixer(place, **arrays):
    arrays = [arrays[name] for name in MIXER_INPUTS]
    at = dict(zip(MIXER_INPUTS, arrays))
    resid, conv_state, scan_state = at["resid"], at["conv_state"], at["scan_state"]
    vmem = pl.BlockSpec(memory_space=pltpu.VMEM)
    hbm = pl.BlockSpec(memory_space=pltpu.HBM)
    scalars = ("step_bias", "decay_rate")
    held = [
        (pltpu.SMEM if name in scalars else pltpu.VMEM)(array.shape, array.dtype)
        for name, array in at.items()
    ]
    return pl.pallas_call(
        mixer_kernel,
        name="mixer",
        in_specs=[pl.BlockSpec(memory_space=pltpu.SMEM)] + [hbm] * len(arrays),
        out_specs=[vmem, hbm, hbm],
        scratch_shapes=held
        + [
            pltpu.VMEM(scan_state.shape, scan_state.dtype),
            pltpu.VMEM(conv_state.shape, conv_state.dtype),
            pltpu.VMEM((scan_state.shape[1], resid.shape[0], scan_state.shape[3]), jnp.float32),
            pltpu.SemaphoreType.DMA((len(arrays),)),
            pltpu.SemaphoreType.DMA((STATE_CHUNKS,)),
            pltpu.SemaphoreType.DMA((STATE_CHUNKS + 1,)),
        ],
        out_shape=[
            jax.ShapeDtypeStruct(resid.shape, jnp.bfloat16),
            jax.ShapeDtypeStruct(scan_state.shape, jnp.float32),
            jax.ShapeDtypeStruct(conv_state.shape, jnp.bfloat16),
        ],
    )(place, *arrays)


def joined_halves(first, second):
    pairs = first.shape[0] // 16
    first = first.reshape(pairs, 2, 8, first.shape[1])
    second = second.reshape(pairs, 2, 8, second.shape[1])
    upper = first[:, 0] + pltpu.roll(second[:, 0], 4, 1)
    lower = pltpu.roll(first[:, 1], 4, 1) + second[:, 1]
    places = lax.broadcasted_iota(jnp.int32, upper.shape, 1)
    return jnp.where(places < 4, upper, lower).reshape(pairs * 8, upper.shape[2])


def expert_in_kernel(*refs):
    rows, gate, up, *downs, hidden, down, sems = refs
    copies = [
        pltpu.make_async_copy(part, down.at[k], sems.at[k]) for k, part in enumerate(downs)
    ]
    for copy in copies:
        copy.start()
    half = gate.shape[0] // 2
    gate_value, up_value = [
        joined_halves(dot32(rows[...], w[:half]), dot32(rows[...], w[half:])) for w in (gate, up)
    ]
    hidden[...] = (silu(gate_value) * up_value).astype(jnp.bfloat16)
    for copy in copies:
        copy.wait()


def expert_in(rows, gate, up, *downs):
    vmem = pl.BlockSpec(memory_space=pltpu.VMEM)
    hbm = pl.BlockSpec(memory_space=pltpu.HBM)
    return pl.pallas_call(
        expert_in_kernel,
        name="expert_in",
        in_specs=[vmem] * 3 + [hbm] * len(downs),
        out_specs=[vmem] * 2,
        compiler_params=pltpu.CompilerParams(vmem_limit_bytes=FEEDER_VMEM),
        scratch_shapes=[pltpu.SemaphoreType.DMA((len(downs),))],
        out_shape=[
            jax.ShapeDtypeStruct((rows.shape[0] // 2, gate.shape[1]), jnp.bfloat16),
            jax.ShapeDtypeStruct((len(downs), *downs[0].shape), jnp.bfloat16),
        ],
    )(rows, gate, up, *downs)


def expert_out_kernel(*refs):
    *parts, down, out = refs
    total = dot32(parts[0][...], down[0])
    for k in range(1, len(parts)):
        total = total + dot32(parts[k][...], down[k])
    out[...] = total.astype(jnp.bfloat16)


def simple_call(kernel, shape, *arrays):
    vmem = pl.BlockSpec(memory_space=pltpu.VMEM)
    return pl.pallas_call(
        kernel,
        in_specs=[vmem] * len(arrays),
        out_specs=vmem,
        compiler_params=pltpu.CompilerParams(vmem_limit_bytes=FEEDER_VMEM),
        out_shape=jax.ShapeDtypeStruct(shape, jnp.bfloat16),
    )(*arrays)


def slots_kernel(routes, in_slot, in_half_slot):
    for out, halves in ((in_slot, 1), (in_half_slot, 2)):
        _, columns = out.shape
        seqs = columns // halves
        slot_ids = lax.broadcasted_iota(jnp.int32, out.shape, 0)
        token_ids = lax.broadcasted_iota(jnp.int32, out.shape, 1)
        picked = jnp.zeros(out.shape, jnp.bool_)
        for k in range(routes.shape[0]):
            picked = picked | ((slot_ids >> (1 + halves)) == routes[k : k + 1, :columns])
        before = lax.broadcasted_iota(jnp.int32, (columns, columns), 0)
        after = lax.broadcasted_iota(jnp.int32, (columns, columns), 1)
        earlier = (before < after) & ((before >= seqs) == (after >= seqs))
        rank = dot32(
            jnp.where(picked, 1.0, 0.0).astype(jnp.bfloat16),
            jnp.where(earlier, 1.0, 0.0).astype(jnp.bfloat16),
        )
        here = picked & (rank.astype(jnp.int32) == (slot_ids & 3))
        if halves == 2:
            here = here & (((slot_ids & 4) != 0) == (token_ids >= seqs))
        out[...] = jnp.where(here, 1.0, 0.0).astype(out.dtype)


def slots_of(slots, routes):
    seqs = routes.shape[1] // 2
    vmem = pl.BlockSpec(memory_space=pltpu.VMEM)
    return pl.pallas_call(
        slots_kernel,
        name="slots",
        in_specs=[vmem],
        out_specs=[vmem] * 2,
        compiler_params=pltpu.CompilerParams(vmem_limit_bytes=FEEDER_VMEM),
        out_shape=[
            jax.ShapeDtypeStruct((slots, seqs), jnp.float32),
            jax.ShapeDtypeStruct((2 * slots, 2 * seqs), jnp.bfloat16),
        ],
    )(routes)


def feeder_kernel(
    place, part_0, part_1, part_2, part_3, resid, post_gain, ffn_gain, in_half_slot,
    kept_out, feed_quarter, rows_out, kept, rows, sems,
):
    mixed = sum_of([part_0[...], part_1[...], part_2[...], part_3[...]])
    total = resid[...].astype(jnp.float32) + scaled_rows(mixed, post_gain[...])
    total = total.astype(jnp.bfloat16)
    fed = scaled_rows(total, ffn_gain[...]).astype(jnp.bfloat16)
    width, quarter = fed.shape[1], feed_quarter.shape[1]
    kept[:, :width] = fed
    for q in range(width // quarter):

        @pl.when(place[0] == q)
        def _(q=q):
            kept[:, width:] = total[:, q * quarter : (q + 1) * quarter]
            feed_quarter[...] = fed[:, q * quarter : (q + 1) * quarter]

    half = fed.shape[1] // 2
    halves = jnp.concatenate([fed[:, :half], fed[:, half:]], axis=0)
    some = rows.shape[0] // ROW_CHUNKS
    copies = []
    for i in range(ROW_CHUNKS):
        chunk = pl.ds(i * some, some)
        rows[chunk] = dot32(in_half_slot[chunk], halves).astype(jnp.bfloat16)
        copies.append(pltpu.make_async_copy(rows.at[chunk], rows_out.at[chunk], sems.at[i]))
        copies[-1].start()
    copies.append(pltpu.make_async_copy(kept, kept_out, sems.at[ROW_CHUNKS]))
    copies[-1].start()
    for copy in copies:
        copy.wait()


def feeder(quarter, place, *arrays):
    vmem = pl.BlockSpec(memory_space=pltpu.VMEM)
    hbm = pl.BlockSpec(memory_space=pltpu.HBM)
    shape = arrays[1].shape
    share, kept = (shape[0], quarter), (shape[0], shape[1] + quarter)
    rows = (arrays[-1].shape[0], shape[1] // 2)
    return pl.pallas_call(
        feeder_kernel,
        name="feeder",
        in_specs=[pl.BlockSpec(memory_space=pltpu.SMEM)] + [vmem] * len(arrays),
        out_specs=[hbm, vmem, hbm],
        compiler_params=pltpu.CompilerParams(vmem_limit_bytes=FEEDER_VMEM),
        scratch_shapes=[pltpu.VMEM(x, jnp.bfloat16) for x in (kept, rows)]
        + [pltpu.SemaphoreType.DMA((ROW_CHUNKS + 1,))],
        out_shape=[jax.ShapeDtypeStruct(x, jnp.bfloat16) for x in (kept, share, rows)],
    )(place, *arrays)


def on_device(
    resid,
    mix_gain,
    proj_x,
    proj_z,
    proj_b,
    proj_c,
    proj_step,
    step_bias,
    decay_rate,
    conv_taps,
    conv_state,
    scan_state,
    inner_gain,
    proj_out,
    post_gain,
    ffn_gain,
    group_router,
    expert_router,
    route_experts,
    expert_gate,
    expert_up,
    expert_down,
    dense_switch,
    dense_gate,
    dense_up,
    dense_down,
    out_gain,
):
    tp_index = lax.axis_index("tp")
    tp_count = lax.axis_size("tp")
    seqs, width = resid.shape
    quarter = width // tp_count
    channels = conv_state.shape[3]
    units = dense_gate.shape[0]

    blocks = jnp.stack([dense_gate, dense_up, dense_down])[None]
    blocks = jnp.concatenate([blocks, from_flip(blocks, "ep_0", 4)])
    blocks = jnp.concatenate([blocks, from_flip(blocks, "ep_0", 2)])
    unit_rows = jnp.moveaxis(blocks, 0, 1).reshape(3, blocks.shape[0] * units, quarter)
    expert_count = expert_router.shape[1]
    group_size = expert_count // group_router.shape[1]
    pick_count = route_experts.shape[1]
    capacity = 2 * seqs * pick_count // expert_count

    place = jnp.full((1,), tp_index, jnp.int32)
    part, new_state, new_conv = mixer(
        place,
        resid=resid,
        mix_gain=mix_gain.reshape(-1, channels),
        proj_x=proj_x,
        proj_b=proj_b,
        proj_c=proj_c,
        proj_step=proj_step.T,
        conv_taps=conv_taps,
        conv_state=conv_state.transpose(1, 2, 0, 3),
        step_bias=step_bias,
        decay_rate=decay_rate,
        scan_state=scan_state,
        proj_z=proj_z,
        inner_gain=inner_gain[None],
        proj_out=proj_out,
    )
    new_conv = new_conv.transpose(2, 0, 1, 3)
    mixed_parts = from_all(part, "tp")
    mixed_parts[0] = part.astype(jnp.float32)
    in_slot, in_half_slot = slots_of(
        expert_count * capacity, jnp.tile(route_experts.T, (1, 2))
    )
    kept, feed_quarter, outgoing = feeder(
        quarter, place, *mixed_parts, resid.astype(jnp.float32), post_gain[None],
        ffn_gain[None], in_half_slot,
    )

    arrived = lax.all_to_all(
        outgoing.reshape(expert_count, 2 * capacity, width // 2), EP, 0, 0, tiled=True
    )
    rows = arrived.reshape(2 * expert_count * capacity, width // 2)

    tokens = lax.optimization_barrier((feed_quarter, from_flip(feed_quarter, "ep_0", 1)))
    tokens = jnp.concatenate(tokens, axis=0)
    tokens = jnp.concatenate(from_all(tokens, "ep_1"), axis=0)
    tokens = jnp.concatenate([tokens, from_flip(tokens, "ep_2", 1)], axis=0)
    kept, tokens = lax.optimization_barrier((kept, tokens))
    feed, stream_quarter = kept[:, :width], kept[:, width:]
    down_rows = unit_rows[2]
    down = expert_down[0]
    down_parts = [
        lax.dynamic_slice_in_dim(down, ((tp_index + s) % tp_count) * quarter, quarter, 1)
        for s in range(tp_count)
    ]
    down_parts = [down_parts[0]] + [from_shift(down_parts[s], "tp", s) for s in range(1, tp_count)]
    across = (((1,), (1,)), ((), ()))
    pieces = lax.dot_general(
        tokens, unit_rows[:2].reshape(-1, quarter), across, preferred_element_type=jnp.float32
    ).astype(jnp.bfloat16)
    sums = from_all(pieces, "tp")

    features = (((0,), (1,)), ((), ()))
    group_exp = jnp.exp(
        lax.dot_general(group_router, feed, features, preferred_element_type=jnp.float32)
    )
    group_prob = group_exp / jnp.sum(group_exp, axis=0, keepdims=True)
    routes = route_experts.T
    group_ids = jnp.arange(group_router.shape[1], dtype=jnp.int32)[:, None]
    group_weight = jnp.sum(
        jnp.where(routes[:1] // group_size == group_ids, group_prob, 0.0), axis=0, keepdims=True
    )
    expert_ids = jnp.arange(expert_count, dtype=jnp.int32)[:, None]
    picked = expert_ids == routes[0:1]
    for k in range(1, pick_count):
        picked = picked | (expert_ids == routes[k : k + 1])
    logits = lax.dot_general(expert_router, feed, features, preferred_element_type=jnp.float32)
    pick_exp = jnp.exp(jnp.where(picked, logits, -jnp.inf))
    pick_weight = pick_exp / jnp.sum(pick_exp, axis=0, keepdims=True) * group_weight
    slot_weight = in_slot * jnp.repeat(pick_weight, capacity, axis=0)
    weight_high = slot_weight.astype(jnp.bfloat16)
    weight_low = (slot_weight - weight_high.astype(jnp.float32)).astype(jnp.bfloat16)
    switch = jax.nn.sigmoid(dot32(feed, dense_switch))
    stream_share = stream_quarter.astype(jnp.float32)
    rows, weight_high, weight_low, switch, stream_share, *down_parts = (
        lax.optimization_barrier(
            (rows, weight_high, weight_low, switch, stream_share, *down_parts)
        )
    )

    hidden, down_rows_here = expert_in(rows, expert_gate[0], expert_up[0], *down_parts)
    _, *sums = lax.optimization_barrier((hidden, *sums))
    hidden_parts = from_all(hidden, "tp")
    sums = sum_of(sums)
    gate_sum, up_sum = jnp.split(sums, 2, axis=1)
    dense_hidden = (jax.nn.silu(gate_sum) * up_sum).astype(jnp.bfloat16)
    dense_part = dot32(dense_hidden, down_rows).astype(jnp.bfloat16)
    half = dense_part.shape[0] // 2
    lots = sum_of([dense_part[:half], from_flip(dense_part[half:], "ep_2", 1)])
    lots = lots.astype(jnp.bfloat16).reshape(lax.axis_size("ep_1"), 2, seqs, quarter)
    lots = sum_of([lots[:, 0], from_flip(lots[:, 1], "ep_0", 1)])
    lots = lots.astype(jnp.bfloat16)
    dense_part = sum_of(
        [lots[0]] + [from_shift(lots[b], "ep_1", -b) for b in range(1, lots.shape[0])]
    )
    dense_out = dense_part

    served = simple_call(
        expert_out_kernel, (rows.shape[0] // 2, quarter), *hidden_parts, down_rows_here
    )
    returned = lax.all_to_all(
        served.reshape(expert_count, capacity, quarter), EP, 0, 0, tiled=True
    ).reshape(expert_count * capacity, quarter)

    slotwise = (((0,), (0,)), ((), ()))
    routed = lax.dot_general(
        weight_high, returned, slotwise, preferred_element_type=jnp.float32
    ) + lax.dot_general(weight_low, returned, slotwise, preferred_element_type=jnp.float32)

    combined = routed + switch[:, None] * dense_out
    squares = jnp.sum(combined * combined, axis=1)
    total_square = sum_of(from_all(squares, "tp"))
    scale = lax.rsqrt(total_square / width + norm_eps)
    layer_out = (stream_share + combined * scale[:, None] * out_gain.astype(jnp.float32)).astype(
        jnp.bfloat16
    )
    return (layer_out, new_state, new_conv)


def solution(mesh):
    torus = Mesh(mesh.devices.reshape(8, 4, 2, mesh.shape["tp"]), ("ep_0", "ep_1", "ep_2", "tp"))
    in_specs = (
        P(EP, None),
        P(),
        P(None, "tp"),
        P(None, "tp"),
        P(None, "tp"),
        P(None, "tp"),
        P(),
        P("tp"),
        P("tp"),
        P(None, None, "tp"),
        P(EP, None, None, "tp"),
        P(EP, "tp", None, None),
        P("tp"),
        P("tp", None),
        P(),
        P(),
        P(),
        P(),
        P(EP, None),
        P(EP, None, "tp"),
        P(EP, None, "tp"),
        P(EP, "tp", None),
        P(),
        P(EP, "tp"),
        P(EP, "tp"),
        P(EP, "tp"),
        P("tp"),
    )
    out_specs = (P(EP, "tp"), P(EP, "tp", None, None), P(EP, None, None, "tp"))

    return jax.shard_map(
        on_device, mesh=torus, in_specs=in_specs, out_specs=out_specs, check_vma=False
    )
```

```python
import jax
import jax.numpy as jnp
from jax import lax
from jax.sharding import Mesh
from jax.experimental import pallas as pl
from jax.experimental.pallas import tpu as pltpu
from jax.sharding import PartitionSpec as P


EP = ("ep_0", "ep_1", "ep_2")


norm_eps = 1e-06
FEEDER_VMEM = 16 * 2**20
STATE_CHUNKS = 4
ROW_CHUNKS = 4


def from_shift(array, axis, shift):
    count = lax.axis_size(axis)
    return lax.ppermute(array, axis, [(i, (i + shift) % count) for i in range(count)])


def from_all(array, axis):
    count = lax.axis_size(axis)
    return [array] + [from_shift(array, axis, s) for s in range(1, count)]


def scaled_rows(values, gain):
    values = values.astype(jnp.float32)
    mean_square = jnp.mean(values * values, axis=-1, keepdims=True)
    return values * lax.rsqrt(mean_square + norm_eps) * gain.astype(jnp.float32)


def dot32(a, b):
    return jnp.dot(a, b, preferred_element_type=jnp.float32)


def sum_of(arrays):
    total = arrays[0].astype(jnp.float32)
    for array in arrays[1:]:
        total = total + array.astype(jnp.float32)
    return total


def from_flip(array, axis, bit):
    count = lax.axis_size(axis)
    return lax.ppermute(array, axis, [(i, i ^ bit) for i in range(count)])


def silu(values):
    return values * (1.0 / (1.0 + jnp.exp(-values)))


MIXER_INPUTS = (
    "resid", "mix_gain", "proj_x", "proj_b", "proj_c", "proj_step", "conv_taps",
    "conv_state", "step_bias", "decay_rate", "scan_state", "proj_z", "inner_gain", "proj_out",
)


def in_two(values):
    high = values.astype(jnp.bfloat16).astype(jnp.float32)
    return high, values - high


def across_last(a, b):
    return lax.dot_general(a, b, (((1,), (1,)), ((), ())), preferred_element_type=jnp.float32)


def mixer_kernel(place, *refs):
    count = len(MIXER_INPUTS)
    sources, refs = refs[:count], refs[count:]
    (part, state_out, conv_out), refs = refs[:3], refs[3:]
    held, refs = refs[:count], refs[count:]
    new_state, new_conv, keep_rows, sems, in_sems, out_sems = refs
    at = dict(zip(MIXER_INPUTS, held))
    scan_state = at["scan_state"]
    copies = {
        name: pltpu.make_async_copy(source, target, sems.at[k])
        for k, (name, source, target) in enumerate(zip(MIXER_INPUTS, sources, held))
        if name != "scan_state"
    }
    state_in = dict(zip(MIXER_INPUTS, sources))["scan_state"]

    def share(i):
        some = state_in.shape[0] // STATE_CHUNKS
        return pl.ds(i * some, some)

    def state_copy(i):
        return pltpu.make_async_copy(
            state_in.at[share(i)], scan_state.at[share(i)], in_sems.at[i]
        )

    def out_copy(i):
        return pltpu.make_async_copy(
            new_state.at[share(i)], state_out.at[share(i)], out_sems.at[i]
        )

    for name in MIXER_INPUTS:
        if name == "scan_state":
            for i in range(STATE_CHUNKS):
                state_copy(i).start()
        else:
            copies[name].start()

    seqs = part.shape[0]
    heads, head_dim, lanes = new_state.shape[1:]
    copies["resid"].wait()
    copies["mix_gain"].wait()
    values = at["resid"][...].astype(jnp.float32)
    mean_square = jnp.mean(values * values, axis=-1, keepdims=True)
    values = values * lax.rsqrt(mean_square + norm_eps)
    gains = at["mix_gain"][...].astype(jnp.float32)
    normed = jnp.concatenate(
        [
            values[:, k * lanes : (k + 1) * lanes] * gains[k : k + 1]
            for k in range(gains.shape[0])
        ],
        axis=1,
    ).astype(jnp.bfloat16)

    raws = []
    for name in ("proj_x", "proj_b", "proj_c"):
        copies[name].wait()
        raws.append(dot32(normed, at[name][...]))
    for name in ("proj_step", "conv_taps", "conv_state", "step_bias", "decay_rate"):
        copies[name].wait()
    conv_state, conv_taps = at["conv_state"], at["conv_taps"]
    parts = []
    for k, raw in enumerate(raws):
        fresh = raw.astype(jnp.bfloat16)
        taps = conv_taps[k].astype(jnp.float32)
        total = fresh.astype(jnp.float32) * taps[3:4]
        for pos in range(3):
            total = total + conv_state[k, pos].astype(jnp.float32) * taps[pos : pos + 1]
        new_conv[k, 0] = conv_state[k, 1]
        new_conv[k, 1] = conv_state[k, 2]
        new_conv[k, 2] = fresh
        parts.append(silu(total))
    conv_copy = pltpu.make_async_copy(new_conv, conv_out, out_sems.at[STATE_CHUNKS])
    conv_copy.start()
    xs, bs, cs = parts
    step_all = lax.dot_general(
        normed, at["proj_step"][...], (((1,), (1,)), ((), ())), preferred_element_type=jnp.float32
    )
    head_ids = lax.broadcasted_iota(jnp.int32, step_all.shape, 1)
    lane_ids = lax.broadcasted_iota(jnp.int32, (seqs, lanes), 1)
    steps, keeps = [], []
    for h in range(heads):
        raw = jnp.sum(
            jnp.where(head_ids == place[0] * heads + h, step_all, 0.0), axis=1, keepdims=True
        )
        raw = raw + at["step_bias"][h]
        step = jnp.maximum(raw, 0.0) + jnp.log1p(jnp.exp(-jnp.abs(raw)))
        steps.append(step)
        keeps.append(jnp.exp(-at["decay_rate"][h] * step))
    driven = xs * jnp.where(lane_ids < head_dim, steps[0], steps[1])
    blank = jnp.zeros((lanes - 3 * seqs, lanes), jnp.float32)
    high, low = in_two(driven)
    columns = jnp.concatenate([high, low, high, blank], axis=0).T
    high, low = in_two(bs)
    b_rows = jnp.concatenate([high, high, low, blank], axis=0).astype(jnp.bfloat16)
    blank = jnp.zeros((lanes - seqs, lanes), jnp.float32)
    c_high, c_low = [
        jnp.concatenate([c, blank], axis=0).astype(jnp.bfloat16) for c in in_two(cs)
    ]
    for h in range(heads):
        keep_rows[h] = jnp.broadcast_to(keeps[h], (seqs, lanes))
    wide_ids = lax.broadcasted_iota(jnp.int32, (heads * head_dim, lanes), 1)
    lots = heads * head_dim
    some = seqs // STATE_CHUNKS

    def chunk(i, read):
        first = pl.multiple_of(i * some, some)
        state_copy(i).wait()
        masked = [
            jnp.where((wide_ids & (seqs - 1)) == first + k, columns, 0.0).astype(jnp.bfloat16)
            for k in range(some)
        ]
        outer = dot32(jnp.concatenate(masked, axis=0), b_rows)
        states = []
        for h in range(heads):
            keep = keep_rows[h, pl.ds(first, some)]
            for k in range(some):
                at_row = k * lots + h * head_dim
                state = (
                    keep[k : k + 1] * scan_state[first + k, h]
                    + outer[at_row : at_row + head_dim]
                )
                new_state[first + k, h] = state
                states.append((at_row, state))
        out_copy(i).start()
        states = jnp.concatenate([state for _, state in sorted(states, key=lambda x: x[0])])
        high, low = [x.astype(jnp.bfloat16) for x in in_two(states)]
        found = across_last(high, c_high) + (across_last(low, c_high) + across_last(high, c_low))
        for k in range(some):
            read = read + jnp.where(
                wide_ids == first + k, found[k * lots : (k + 1) * lots], 0.0
            )
        return read

    read = lax.fori_loop(0, STATE_CHUNKS, chunk, jnp.zeros((lots, lanes), jnp.float32))
    read = read.T[:seqs]
    copies["proj_z"].wait()
    copies["inner_gain"].wait()
    gate = silu(dot32(normed, at["proj_z"][...])) * at["inner_gain"][...].astype(jnp.float32)
    gated = (read * gate).astype(jnp.bfloat16)
    copies["proj_out"].wait()
    part[...] = dot32(gated, at["proj_out"][...]).astype(jnp.bfloat16)
    for i in range(STATE_CHUNKS):
        out_copy(i).wait()
    conv_copy.wait()


def mixer(place, **arrays):
    arrays = [arrays[name] for name in MIXER_INPUTS]
    at = dict(zip(MIXER_INPUTS, arrays))
    resid, conv_state, scan_state = at["resid"], at["conv_state"], at["scan_state"]
    vmem = pl.BlockSpec(memory_space=pltpu.VMEM)
    hbm = pl.BlockSpec(memory_space=pltpu.HBM)
    scalars = ("step_bias", "decay_rate")
    held = [
        (pltpu.SMEM if name in scalars else pltpu.VMEM)(array.shape, array.dtype)
        for name, array in at.items()
    ]
    return pl.pallas_call(
        mixer_kernel,
        name="mixer",
        in_specs=[pl.BlockSpec(memory_space=pltpu.SMEM)] + [hbm] * len(arrays),
        out_specs=[vmem, hbm, hbm],
        scratch_shapes=held
        + [
            pltpu.VMEM(scan_state.shape, scan_state.dtype),
            pltpu.VMEM(conv_state.shape, conv_state.dtype),
            pltpu.VMEM((scan_state.shape[1], resid.shape[0], scan_state.shape[3]), jnp.float32),
            pltpu.SemaphoreType.DMA((len(arrays),)),
            pltpu.SemaphoreType.DMA((STATE_CHUNKS,)),
            pltpu.SemaphoreType.DMA((STATE_CHUNKS + 1,)),
        ],
        out_shape=[
            jax.ShapeDtypeStruct(resid.shape, jnp.bfloat16),
            jax.ShapeDtypeStruct(scan_state.shape, jnp.float32),
            jax.ShapeDtypeStruct(conv_state.shape, jnp.bfloat16),
        ],
    )(place, *arrays)


def joined_halves(first, second):
    pairs = first.shape[0] // 16
    first = first.reshape(pairs, 2, 8, first.shape[1])
    second = second.reshape(pairs, 2, 8, second.shape[1])
    upper = first[:, 0] + pltpu.roll(second[:, 0], 4, 1)
    lower = pltpu.roll(first[:, 1], 4, 1) + second[:, 1]
    places = lax.broadcasted_iota(jnp.int32, upper.shape, 1)
    return jnp.where(places < 4, upper, lower).reshape(pairs * 8, upper.shape[2])


def expert_in_kernel(*refs):
    rows, gate, up, *downs, hidden, down, sems = refs
    copies = [
        pltpu.make_async_copy(part, down.at[k], sems.at[k]) for k, part in enumerate(downs)
    ]
    for copy in copies:
        copy.start()
    half = gate.shape[0] // 2
    gate_value, up_value = [
        joined_halves(dot32(rows[...], w[:half]), dot32(rows[...], w[half:])) for w in (gate, up)
    ]
    hidden[...] = (silu(gate_value) * up_value).astype(jnp.bfloat16)
    for copy in copies:
        copy.wait()


def expert_in(rows, gate, up, *downs):
    vmem = pl.BlockSpec(memory_space=pltpu.VMEM)
    hbm = pl.BlockSpec(memory_space=pltpu.HBM)
    return pl.pallas_call(
        expert_in_kernel,
        name="expert_in",
        in_specs=[vmem] * 3 + [hbm] * len(downs),
        out_specs=[vmem] * 2,
        compiler_params=pltpu.CompilerParams(vmem_limit_bytes=FEEDER_VMEM),
        scratch_shapes=[pltpu.SemaphoreType.DMA((len(downs),))],
        out_shape=[
            jax.ShapeDtypeStruct((rows.shape[0] // 2, gate.shape[1]), jnp.bfloat16),
            jax.ShapeDtypeStruct((len(downs), *downs[0].shape), jnp.bfloat16),
        ],
    )(rows, gate, up, *downs)


def expert_out_kernel(*refs):
    *parts, down, out = refs
    total = dot32(parts[0][...], down[0])
    for k in range(1, len(parts)):
        total = total + dot32(parts[k][...], down[k])
    out[...] = total.astype(jnp.bfloat16)


def simple_call(kernel, shape, *arrays):
    vmem = pl.BlockSpec(memory_space=pltpu.VMEM)
    return pl.pallas_call(
        kernel,
        in_specs=[vmem] * len(arrays),
        out_specs=vmem,
        compiler_params=pltpu.CompilerParams(vmem_limit_bytes=FEEDER_VMEM),
        out_shape=jax.ShapeDtypeStruct(shape, jnp.bfloat16),
    )(*arrays)


def slots_kernel(routes, in_slot, in_half_slot):
    for out, halves in ((in_slot, 1), (in_half_slot, 2)):
        _, columns = out.shape
        seqs = columns // halves
        slot_ids = lax.broadcasted_iota(jnp.int32, out.shape, 0)
        token_ids = lax.broadcasted_iota(jnp.int32, out.shape, 1)
        picked = jnp.zeros(out.shape, jnp.bool_)
        for k in range(routes.shape[0]):
            picked = picked | ((slot_ids >> (1 + halves)) == routes[k : k + 1, :columns])
        before = lax.broadcasted_iota(jnp.int32, (columns, columns), 0)
        after = lax.broadcasted_iota(jnp.int32, (columns, columns), 1)
        earlier = (before < after) & ((before >= seqs) == (after >= seqs))
        rank = dot32(
            jnp.where(picked, 1.0, 0.0).astype(jnp.bfloat16),
            jnp.where(earlier, 1.0, 0.0).astype(jnp.bfloat16),
        )
        here = picked & (rank.astype(jnp.int32) == (slot_ids & 3))
        if halves == 2:
            here = here & (((slot_ids & 4) != 0) == (token_ids >= seqs))
        out[...] = jnp.where(here, 1.0, 0.0).astype(out.dtype)


def slots_of(slots, routes):
    seqs = routes.shape[1] // 2
    vmem = pl.BlockSpec(memory_space=pltpu.VMEM)
    return pl.pallas_call(
        slots_kernel,
        name="slots",
        in_specs=[vmem],
        out_specs=[vmem] * 2,
        compiler_params=pltpu.CompilerParams(vmem_limit_bytes=FEEDER_VMEM),
        out_shape=[
            jax.ShapeDtypeStruct((slots, seqs), jnp.bfloat16),
            jax.ShapeDtypeStruct((2 * slots, 2 * seqs), jnp.bfloat16),
        ],
    )(routes)


def feeder_kernel(
    place, part_0, part_1, part_2, part_3, resid, post_gain, ffn_gain, in_half_slot,
    kept_out, feed_quarter, rows_out, kept, rows, sems,
):
    mixed = sum_of([part_0[...], part_1[...], part_2[...], part_3[...]])
    total = resid[...].astype(jnp.float32) + scaled_rows(mixed, post_gain[...])
    total = total.astype(jnp.bfloat16)
    fed = scaled_rows(total, ffn_gain[...]).astype(jnp.bfloat16)
    width, quarter = fed.shape[1], feed_quarter.shape[1]
    kept[:, :width] = fed
    for q in range(width // quarter):

        @pl.when(place[0] == q)
        def _(q=q):
            kept[:, width:] = total[:, q * quarter : (q + 1) * quarter]
            feed_quarter[...] = fed[:, q * quarter : (q + 1) * quarter]

    half = fed.shape[1] // 2
    halves = jnp.concatenate([fed[:, :half], fed[:, half:]], axis=0)
    some = rows.shape[0] // ROW_CHUNKS
    copies = []
    for i in range(ROW_CHUNKS):
        chunk = pl.ds(i * some, some)
        rows[chunk] = dot32(in_half_slot[chunk], halves).astype(jnp.bfloat16)
        copies.append(pltpu.make_async_copy(rows.at[chunk], rows_out.at[chunk], sems.at[i]))
        copies[-1].start()
    copies.append(pltpu.make_async_copy(kept, kept_out, sems.at[ROW_CHUNKS]))
    copies[-1].start()
    for copy in copies:
        copy.wait()


def feeder(quarter, place, *arrays):
    vmem = pl.BlockSpec(memory_space=pltpu.VMEM)
    hbm = pl.BlockSpec(memory_space=pltpu.HBM)
    shape = arrays[1].shape
    share, kept = (shape[0], quarter), (shape[0], shape[1] + quarter)
    rows = (arrays[-1].shape[0], shape[1] // 2)
    return pl.pallas_call(
        feeder_kernel,
        name="feeder",
        in_specs=[pl.BlockSpec(memory_space=pltpu.SMEM)] + [vmem] * len(arrays),
        out_specs=[hbm, vmem, hbm],
        compiler_params=pltpu.CompilerParams(vmem_limit_bytes=FEEDER_VMEM),
        scratch_shapes=[pltpu.VMEM(x, jnp.bfloat16) for x in (kept, rows)]
        + [pltpu.SemaphoreType.DMA((ROW_CHUNKS + 1,))],
        out_shape=[jax.ShapeDtypeStruct(x, jnp.bfloat16) for x in (kept, share, rows)],
    )(place, *arrays)


def on_device(
    resid,
    mix_gain,
    proj_x,
    proj_z,
    proj_b,
    proj_c,
    proj_step,
    step_bias,
    decay_rate,
    conv_taps,
    conv_state,
    scan_state,
    inner_gain,
    proj_out,
    post_gain,
    ffn_gain,
    group_router,
    expert_router,
    route_experts,
    expert_gate,
    expert_up,
    expert_down,
    dense_switch,
    dense_gate,
    dense_up,
    dense_down,
    out_gain,
):
    tp_index = lax.axis_index("tp")
    tp_count = lax.axis_size("tp")
    seqs, width = resid.shape
    quarter = width // tp_count
    channels = conv_state.shape[3]
    units = dense_gate.shape[0]

    blocks = jnp.stack([dense_gate, dense_up, dense_down])[None]
    blocks = jnp.concatenate([blocks, from_flip(blocks, "ep_0", 4)])
    blocks = jnp.concatenate([blocks, from_flip(blocks, "ep_0", 2)])
    unit_rows = jnp.moveaxis(blocks, 0, 1).reshape(3, blocks.shape[0] * units, quarter)
    expert_count = expert_router.shape[1]
    group_size = expert_count // group_router.shape[1]
    pick_count = route_experts.shape[1]
    capacity = 2 * seqs * pick_count // expert_count

    place = jnp.full((1,), tp_index, jnp.int32)
    part, new_state, new_conv = mixer(
        place,
        resid=resid,
        mix_gain=mix_gain.reshape(-1, channels),
        proj_x=proj_x,
        proj_b=proj_b,
        proj_c=proj_c,
        proj_step=proj_step.T,
        conv_taps=conv_taps,
        conv_state=conv_state.transpose(1, 2, 0, 3),
        step_bias=step_bias,
        decay_rate=decay_rate,
        scan_state=scan_state,
        proj_z=proj_z,
        inner_gain=inner_gain[None],
        proj_out=proj_out,
    )
    new_conv = new_conv.transpose(2, 0, 1, 3)
    mixed_parts = from_all(part, "tp")
    mixed_parts[0] = part.astype(jnp.float32)
    in_slot, in_half_slot = slots_of(
        expert_count * capacity, jnp.tile(route_experts.T, (1, 2))
    )
    kept, feed_quarter, outgoing = feeder(
        quarter, place, *mixed_parts, resid.astype(jnp.float32), post_gain[None],
        ffn_gain[None], in_half_slot,
    )

    arrived = lax.all_to_all(
        outgoing.reshape(expert_count, 2 * capacity, width // 2), EP, 0, 0, tiled=True
    )
    rows = arrived.reshape(2 * expert_count * capacity, width // 2)

    tokens = lax.optimization_barrier((feed_quarter, from_flip(feed_quarter, "ep_0", 1)))
    tokens = jnp.concatenate(tokens, axis=0)
    tokens = jnp.concatenate(from_all(tokens, "ep_1"), axis=0)
    tokens = jnp.concatenate([tokens, from_flip(tokens, "ep_2", 1)], axis=0)
    feed, stream_quarter = kept[:, :width], kept[:, width:]
    down_rows = unit_rows[2]
    down = expert_down[0]
    down_parts = [
        lax.dynamic_slice_in_dim(down, ((tp_index + s) % tp_count) * quarter, quarter, 1)
        for s in range(tp_count)
    ]
    down_parts = [down_parts[0]] + [from_shift(down_parts[s], "tp", s) for s in range(1, tp_count)]
    across = (((1,), (1,)), ((), ()))
    pieces = lax.dot_general(
        tokens, unit_rows[:2].reshape(-1, quarter), across, preferred_element_type=jnp.float32
    ).astype(jnp.bfloat16)
    sums = from_all(pieces, "tp")

    features = (((0,), (1,)), ((), ()))
    group_exp = jnp.exp(
        lax.dot_general(group_router, feed, features, preferred_element_type=jnp.float32)
    )
    group_prob = group_exp / jnp.sum(group_exp, axis=0, keepdims=True)
    routes = route_experts.T
    group_ids = jnp.arange(group_router.shape[1], dtype=jnp.int32)[:, None]
    group_weight = jnp.sum(
        jnp.where(routes[:1] // group_size == group_ids, group_prob, 0.0), axis=0, keepdims=True
    )
    expert_ids = jnp.arange(expert_count, dtype=jnp.int32)[:, None]
    picked = expert_ids == routes[0:1]
    for k in range(1, pick_count):
        picked = picked | (expert_ids == routes[k : k + 1])
    logits = lax.dot_general(expert_router, feed, features, preferred_element_type=jnp.float32)
    pick_exp = jnp.exp(jnp.where(picked, logits, -jnp.inf))
    pick_weight = pick_exp / jnp.sum(pick_exp, axis=0, keepdims=True) * group_weight
    slot_weight = in_slot.astype(jnp.float32) * jnp.repeat(pick_weight, capacity, axis=0)
    weight_high = slot_weight.astype(jnp.bfloat16)
    weight_low = (slot_weight - weight_high.astype(jnp.float32)).astype(jnp.bfloat16)
    switch = jax.nn.sigmoid(dot32(feed, dense_switch))
    stream_share = stream_quarter.astype(jnp.float32)
    rows, weight_high, weight_low, switch, stream_share, *down_parts = (
        lax.optimization_barrier(
            (rows, weight_high, weight_low, switch, stream_share, *down_parts)
        )
    )

    hidden, down_rows_here = expert_in(rows, expert_gate[0], expert_up[0], *down_parts)
    _, *sums = lax.optimization_barrier((hidden, *sums))
    hidden_parts = from_all(hidden, "tp")
    sums = sum_of(sums)
    gate_sum, up_sum = jnp.split(sums, 2, axis=1)
    dense_hidden = (jax.nn.silu(gate_sum) * up_sum).astype(jnp.bfloat16)
    dense_part = dot32(dense_hidden, down_rows).astype(jnp.bfloat16)
    half = dense_part.shape[0] // 2
    lots = sum_of([dense_part[:half], from_flip(dense_part[half:], "ep_2", 1)])
    lots = lots.astype(jnp.bfloat16).reshape(lax.axis_size("ep_1"), 2, seqs, quarter)
    lots = sum_of([lots[:, 0], from_flip(lots[:, 1], "ep_0", 1)])
    lots = lots.astype(jnp.bfloat16)
    dense_part = sum_of(
        [lots[0]] + [from_shift(lots[b], "ep_1", -b) for b in range(1, lots.shape[0])]
    )
    dense_out = dense_part

    served = simple_call(
        expert_out_kernel, (rows.shape[0] // 2, quarter), *hidden_parts, down_rows_here
    )
    returned = lax.all_to_all(
        served.reshape(expert_count, capacity, quarter), EP, 0, 0, tiled=True
    ).reshape(expert_count * capacity, quarter)

    slotwise = (((0,), (0,)), ((), ()))
    routed = lax.dot_general(
        weight_high, returned, slotwise, preferred_element_type=jnp.float32
    ) + lax.dot_general(weight_low, returned, slotwise, preferred_element_type=jnp.float32)

    combined = routed + switch[:, None] * dense_out
    squares = jnp.sum(combined * combined, axis=1)
    total_square = sum_of(from_all(squares, "tp"))
    scale = lax.rsqrt(total_square / width + norm_eps)
    layer_out = (stream_share + combined * scale[:, None] * out_gain.astype(jnp.float32)).astype(
        jnp.bfloat16
    )
    return (layer_out, new_state, new_conv)


def solution(mesh):
    torus = Mesh(mesh.devices.reshape(8, 4, 2, mesh.shape["tp"]), ("ep_0", "ep_1", "ep_2", "tp"))
    in_specs = (
        P(EP, None),
        P(),
        P(None, "tp"),
        P(None, "tp"),
        P(None, "tp"),
        P(None, "tp"),
        P(),
        P("tp"),
        P("tp"),
        P(None, None, "tp"),
        P(EP, None, None, "tp"),
        P(EP, "tp", None, None),
        P("tp"),
        P("tp", None),
        P(),
        P(),
        P(),
        P(),
        P(EP, None),
        P(EP, None, "tp"),
        P(EP, None, "tp"),
        P(EP, "tp", None),
        P(),
        P(EP, "tp"),
        P(EP, "tp"),
        P(EP, "tp"),
        P("tp"),
    )
    out_specs = (P(EP, "tp"), P(EP, "tp", None, None), P(EP, None, None, "tp"))

    return jax.shard_map(
        on_device, mesh=torus, in_specs=in_specs, out_specs=out_specs, check_vma=False
    )
```
